32 devices in a mesh: sp: 8 (over z, y), tp: 4 (over x, core).
Axes of the slice: x: 2, y: 2, z: 4, core: 2. Of those that a mesh axis runs over, the one named last changes fastest.
Arguments:
- query_first: bfloat16 [2048, 512], P('sp', 'tp'), may hold values from -6 to 6
- key_first: bfloat16 [2048, 512], P('sp', 'tp'), may hold values from -6 to 6
- value_first: bfloat16 [2048, 1024], P('sp', 'tp'), may hold values from -6 to 6
- decay_first: float32 [2048, 512], P('sp', 'tp'), may hold values from -1 to 0
- gate_first: bfloat16 [2048, 1024], P('sp', 'tp'), may hold values from -6 to 6
- norm_first: float32 [256], replicated, may hold values from 0.1 to 1.9
- proj_first: bfloat16 [1024, 2048], P('tp', 'sp'), may hold values from -0.125 to 0.125
- query_second: bfloat16 [2048, 512], P('sp', 'tp'), may hold values from -6 to 6
- key_second: bfloat16 [2048, 512], P('sp', 'tp'), may hold values from -6 to 6
- value_second: bfloat16 [2048, 1024], P('sp', 'tp'), may hold values from -6 to 6
- decay_second: float32 [2048, 512], P('sp', 'tp'), may hold values from -1 to 0
- gate_second: bfloat16 [2048, 1024], P('sp', 'tp'), may hold values from -6 to 6
- norm_second: float32 [128], replicated, may hold values from 0.1 to 1.9
- proj_second: bfloat16 [1024, 2048], P('tp', 'sp'), may hold values from -0.125 to 0.125
- residual_in: bfloat16 [2048, 2048], P(('sp', 'tp')), may hold values from -6 to 6
- expert_norm: float32 [2048], replicated, may hold values from 0.1 to 1.9
- route_ids: int32 [2048, 2], P('sp'), may hold values from 0 to 7, all different within a row; in each aligned block of 256 rows (0 to 255, 256 to 511, ...) at most 128 rows name the same one
- route_weight: float32 [2048, 2], P('sp'), may hold values from 0.1 to 0.9
- expert_gate: bfloat16 [8, 2048, 3584], P('sp', None, 'tp'), may hold values from -0.125 to 0.125
- expert_up: bfloat16 [8, 2048, 3584], P('sp', None, 'tp'), may hold values from -0.125 to 0.125
- expert_down: bfloat16 [8, 3584, 2048], P('sp', 'tp'), may hold values from -0.09375 to 0.09375
Outputs:
- layer_out: bfloat16 [2048, 2048], P(('sp', 'tp'))
The draws below stay inside these ranges and needn't reach their ends.
Inputs may be any that keep to these rules, and one draw needn't show every extreme that they name: `route_ids`: each row names 2 different experts. Among the 256 rows of one index of sp no expert is named by more than 128 rows, and in every draw some expert is named by exactly 128 of them.
All inputs are finite; a program needn't handle non-finite values.
Results may differ from the reference program's by a relative error of at most 0.015.
Values may be sent and summed in bfloat16 or wider, within the bound.
A program may use at most 64 MiB of HBM per device.

```python
import math
import jax
import jax.numpy as jnp
import numpy as np
from jax import lax

D = 2048
FF = 3584
HEADS_A = 4
KA = 128
VA = 256
HEADS_B = 8
KB = 64
VB = 128
TOPK = 2
BLK = 64
TOK_DEV = 256
TOKENS = 2048
EXPERTS = 8
CAP = 128
N_TP = 4


def decay_draw(key, count_of_tokens, feature_channels):
    random_subkeys = jax.random.split(key, 7)
    slow_share = 0.5
    gradual_mask = jax.random.uniform(random_subkeys[0], (feature_channels,), jnp.float32) < slow_share
    fast_rates = jnp.exp(jax.random.uniform(random_subkeys[1], (feature_channels,), jnp.float32, jnp.log(1.0 / 60.0), jnp.log(1.0 / 30.0)))
    slow_rates = jnp.exp(jax.random.uniform(random_subkeys[2], (feature_channels,), jnp.float32, jnp.log(0.05 / count_of_tokens), jnp.log(0.3 / count_of_tokens)))
    rates = jnp.where(gradual_mask, slow_rates, fast_rates)
    shard_factor = jnp.exp(jax.random.uniform(random_subkeys[3], (count_of_tokens // TOK_DEV,), jnp.float32, jnp.log(0.5), jnp.log(2.0)))
    shard_factor = jnp.repeat(shard_factor, TOK_DEV)
    roughness = jnp.exp(0.5 * jnp.clip(jax.random.normal(random_subkeys[4], (count_of_tokens, feature_channels), jnp.float32), -2.5, 2.5))
    decay_factors = -rates[None, :] * shard_factor[:, None] * roughness
    spike_position = jax.random.randint(random_subkeys[5], (3,), 0, count_of_tokens)
    spike_found = jnp.any(jnp.arange(count_of_tokens)[:, None] == spike_position[None, :], axis=1)
    spike_penalty = jnp.log(jax.random.uniform(random_subkeys[6], (feature_channels,), jnp.float32, 0.6, 0.8))
    decay_factors = decay_factors + jnp.where(spike_found[:, None] & gradual_mask[None, :], spike_penalty[None, :], 0.0)
    return decay_factors.astype(jnp.float32)


def draw_decay_first(key, part):
    return decay_draw(jax.random.fold_in(key, 11), TOKENS, HEADS_A * KA)


def draw_decay_second(key, part):
    return decay_draw(jax.random.fold_in(key, 23), TOKENS, HEADS_B * KB)


def block_levels(stream_key, extent, shards, low, top_value):
    def one(axis_at, parts):
        draws = jax.random.uniform(jax.random.fold_in(jax.random.fold_in(stream_key, 6), axis_at), (parts,), jnp.float32, low / len(shards), top_value / len(shards))
        return jnp.repeat(jnp.exp(draws), extent[axis_at] // parts).reshape((-1,) + (1,) * (len(extent) - axis_at - 1))

    factor_of = one(*shards[0])
    for cut in shards[1:]:
        factor_of = factor_of * one(*cut)
    return factor_of


def routed_block(rng, own, number, rows, amount, top, most, skew):
    order = jax.random.permutation(rng, amount)
    packed, ordinary = load_shares(amount, rows * top, most, skew, True), load_shares(amount, rows * top, most, skew, False)
    places = jnp.arange(amount)

    def named(sizes, offset_by):
        used = int((sizes > 0).sum())
        fixed = max(1, used // 4)
        shifted = fixed + (places - fixed + offset_by * (used - fixed)) % max(1, amount - fixed)
        return jnp.zeros((amount,), jnp.int32).at[order[jnp.where(places < fixed, places, shifted)]].set(jnp.asarray(sizes, jnp.int32))

    sizes = jnp.where(number % 4 == 0, named(packed, number // 4), named(ordinary, number - number // 4 - 1))
    mixed = jax.random.permutation(jax.random.fold_in(own, 3), amount)
    giver, receiver = mixed[0:amount // 2 * 2:2], mixed[1:amount // 2 * 2:2]
    slack = jnp.minimum(sizes[giver] - 1, most - sizes[receiver]) // 2
    slack = jnp.where((giver == order[0]) | (receiver == order[0]) | (sizes[receiver] == 0), 0, jnp.maximum(slack, 0))
    shifted = jax.random.randint(jax.random.fold_in(own, 4), (amount // 2,), 0, 1 << 20) % (slack + 1)
    sizes = sizes.at[giver].add(-shifted).at[receiver].add(shifted)
    labels = jnp.searchsorted(jnp.cumsum(sizes), jnp.arange(rows * top), side="right").astype(jnp.int32)
    grid = labels.reshape(top, rows).T
    grid = grid[jax.random.permutation(jax.random.fold_in(own, 1), rows)]
    offset_by = jax.random.randint(jax.random.fold_in(own, 2), (rows, 1), 0, top)
    return jnp.take_along_axis(grid, (jnp.arange(top)[None, :] + offset_by) % top, axis=1)


def load_shares(amount, total, most, skew, full):
    portions = [(1 << 20) // math.isqrt(grade ** skew) + 1 for grade in range(1, amount + 1)]
    largest = most if full else min(most, max(-(-total // amount), total * portions[0] // sum(portions)))
    least = 1 if total - largest >= amount - 1 else 0
    holding, surplus = [largest] + [least] * (amount - 1), total - largest - least * (amount - 1)
    while surplus > 0:
        candidates = [i for i in range(1, amount) if holding[i] < largest] or [i for i in range(1, amount) if holding[i] < most]
        mass, remaining = sum([portions[i] for i in candidates]), surplus
        for i in candidates:
            more = min(most - holding[i], max(1, remaining * portions[i] // mass), surplus)
            holding[i] = holding[i] + more
            surplus = surplus - more
    return np.array(holding)


def scatter_about(own_key, shape, deviation, reach, shards=(), held_as=jnp.bfloat16):
    gain = block_levels(own_key, shape, shards, -0.22, 0.18) if shards else 1.0
    entries = jax.random.normal(own_key, shape, jnp.float32) * deviation * gain
    return jnp.minimum(jnp.maximum(entries, -reach), reach).astype(held_as)


def setup_inputs(seed: int = 0) -> dict:
    arg_keys = jax.random.split(jax.random.key(seed), 22)
    query_first = scatter_about(arg_keys[0], (TOKENS, HEADS_A * KA), 1.0, 6.0, ((0, 8), (1, 4)))
    key_first = scatter_about(arg_keys[1], (TOKENS, HEADS_A * KA), 1.0, 6.0, ((0, 8), (1, 4)))
    value_first = scatter_about(arg_keys[2], (TOKENS, HEADS_A * VA), 1.0, 6.0, ((0, 8), (1, 4)))
    decay_first = draw_decay_first(jax.random.fold_in(arg_keys[21], 71), 0)
    gate_first = scatter_about(arg_keys[4], (TOKENS, HEADS_A * VA), 1.0, 6.0, ((0, 8), (1, 4)))
    norm_first = jnp.clip(1.0 + 0.18 * jax.random.normal(arg_keys[5], (VA,), jnp.float32), 0.1, 1.9)
    proj_first = scatter_about(arg_keys[6], (HEADS_A * VA, D), (HEADS_A * VA + HEADS_B * VB) ** -0.5, 0.125, ((0, 4), (1, 8)))
    query_second = scatter_about(arg_keys[7], (TOKENS, HEADS_B * KB), 1.0, 6.0, ((0, 8), (1, 4)))
    key_second = scatter_about(arg_keys[8], (TOKENS, HEADS_B * KB), 1.0, 6.0, ((0, 8), (1, 4)))
    value_second = scatter_about(arg_keys[9], (TOKENS, HEADS_B * VB), 1.0, 6.0, ((0, 8), (1, 4)))
    decay_second = draw_decay_second(jax.random.fold_in(arg_keys[21], 71), 0)
    gate_second = scatter_about(arg_keys[11], (TOKENS, HEADS_B * VB), 1.0, 6.0, ((0, 8), (1, 4)))
    norm_second = jnp.clip(1.0 + 0.18 * jax.random.normal(arg_keys[12], (VB,), jnp.float32), 0.1, 1.9)
    proj_second = scatter_about(arg_keys[13], (HEADS_B * VB, D), (HEADS_A * VA + HEADS_B * VB) ** -0.5, 0.125, ((0, 4), (1, 8)))
    residual_in = scatter_about(arg_keys[14], (TOKENS, D), 1.0, 6.0, ((0, 32),))
    expert_norm = jnp.clip(1.0 + 0.18 * jax.random.normal(arg_keys[15], (D,), jnp.float32), 0.1, 1.9)
    route_ids_keys = jax.random.split(jax.random.fold_in(arg_keys[16], 1), TOKENS // TOK_DEV)
    route_ids_turns = jax.random.permutation(jax.random.fold_in(arg_keys[16], 3), TOKENS // TOK_DEV)
    route_ids = jax.vmap(lambda own, number: routed_block(jax.random.fold_in(arg_keys[16], 2), own, number, TOK_DEV, EXPERTS, TOPK, CAP, 1))(route_ids_keys, route_ids_turns).reshape((TOKENS, TOPK))
    route_weight = jnp.clip(0.1 + 0.79999997 * jax.random.uniform(arg_keys[17], (TOKENS, TOPK), jnp.float32) ** block_levels(arg_keys[17], (TOKENS, TOPK), ((0, 8),), -0.2, 0.2), 0.1, 0.9)
    expert_gate = scatter_about(arg_keys[18], (EXPERTS, D, FF), D ** -0.5, 0.125, ((0, 8), (2, 4)))
    expert_up = scatter_about(arg_keys[19], (EXPERTS, D, FF), D ** -0.5, 0.125, ((0, 8), (2, 4)))
    expert_down = scatter_about(arg_keys[20], (EXPERTS, FF, D), FF ** -0.5, 0.09375, ((0, 8), (1, 4)))
    return dict(query_first=query_first, key_first=key_first, value_first=value_first, decay_first=decay_first, gate_first=gate_first, norm_first=norm_first, proj_first=proj_first, query_second=query_second, key_second=key_second, value_second=value_second, decay_second=decay_second, gate_second=gate_second, norm_second=norm_second, proj_second=proj_second, residual_in=residual_in, expert_norm=expert_norm, route_ids=route_ids, route_weight=route_weight, expert_gate=expert_gate, expert_up=expert_up, expert_down=expert_down)


epsilon = 1e-06
highest = lax.Precision.HIGHEST

def attend(queries, key_rows, values, decay_factors, key_width, value_width):
    count_of_tokens = queries.shape[0]
    head_count = queries.shape[1] // key_width
    blocks = count_of_tokens // BLK

    def arrange(source, feature_channels):
        return source.astype(jnp.float32).reshape(blocks, BLK, head_count, feature_channels).transpose(0, 2, 1, 3)
    causal = jnp.tril(jnp.ones((BLK, BLK), jnp.float32))

    def block_step(carry_state, inputs):
        query_block, key_block, value_block, decay_block = inputs
        cumulative = jnp.cumsum(decay_block, axis=1)
        block_end = cumulative[:, -1:, :]
        query_decayed = query_block * jnp.exp(cumulative)
        key_inverse = key_block * jnp.exp(-cumulative)
        key_to_end = key_block * jnp.exp(block_end - cumulative)
        scores = jnp.einsum('htd,hsd->hts', query_decayed, key_inverse, precision=highest) * causal
        outputs = jnp.einsum('hts,hsv->htv', scores, value_block, precision=highest)
        outputs = outputs + jnp.einsum('htd,hdv->htv', query_decayed, carry_state, precision=highest)
        carry_state = jnp.exp(block_end)[:, 0, :, None] * carry_state + jnp.einsum('hsd,hsv->hdv', key_to_end, value_block, precision=highest)
        return (carry_state, outputs)
    start_state = jnp.zeros((head_count, key_width, value_width), jnp.float32)
    scaled = arrange(queries, key_width) * key_width ** (-0.5)
    end_state, outputs = lax.scan(block_step, start_state, (scaled, arrange(key_rows, key_width), arrange(values, value_width), arrange(decay_factors, key_width)))
    return outputs.transpose(0, 2, 1, 3).reshape(count_of_tokens, head_count, value_width)

def head_norm(attention, head_gain, gate):
    inverse_rms = lax.rsqrt(lax.optimization_barrier(jnp.mean(attention * attention, axis=-1, keepdims=True)) + epsilon)
    gate_silu = jax.nn.silu(gate.astype(jnp.float32).reshape(attention.shape))
    mixed_rows = attention * inverse_rms * head_gain.astype(jnp.float32) * gate_silu
    return mixed_rows.astype(jnp.bfloat16).reshape(attention.shape[0], -1)

def route_tables(block_routes):
    flattened = block_routes.reshape(-1)
    onehot = (flattened[:, None] == jnp.arange(EXPERTS, dtype=jnp.int32)[None, :]).astype(jnp.int32)
    before = (jnp.cumsum(onehot, axis=0) - onehot).astype(jnp.int32)
    ranking = lax.optimization_barrier(jnp.sum(before * onehot, axis=1)).astype(jnp.int32)
    slot_ids = (flattened * CAP + ranking).astype(jnp.int32)
    row_token = (jnp.arange(TOK_DEV * TOPK, dtype=jnp.int32) // TOPK).astype(jnp.int32)
    owners = jnp.full((EXPERTS * CAP,), TOK_DEV, jnp.int32).at[slot_ids].set(row_token)
    return (owners, slot_ids)

def place_weights(slot_ids, weights):
    return jnp.zeros((EXPERTS * CAP,), jnp.float32).at[slot_ids].set(weights.astype(jnp.float32))

def pick_rows(block_rows, index_list):
    return jnp.take(block_rows, index_list, axis=0)

def reference(query_first, key_first, value_first, decay_first, gate_first, norm_first, proj_first, query_second, key_second, value_second, decay_second, gate_second, norm_second, proj_second, residual_in, expert_norm, route_ids, route_weight, expert_gate, expert_up, expert_down):
    attention_first = attend(query_first, key_first, value_first, decay_first, KA, VA)
    attention_second = attend(query_second, key_second, value_second, decay_second, KB, VB)
    mixed_first = head_norm(attention_first, norm_first, gate_first)
    mixed_second = head_norm(attention_second, norm_second, gate_second)
    rows_first = HEADS_A // N_TP * VA
    rows_second = HEADS_B // N_TP * VB
    mixture = jnp.zeros((TOKENS, D), jnp.float32)
    for portion in range(N_TP):
        portion_sum = jnp.dot(mixed_first[:, portion * rows_first:(portion + 1) * rows_first], proj_first[portion * rows_first:(portion + 1) * rows_first], preferred_element_type=jnp.float32)
        portion_sum = portion_sum + jnp.dot(mixed_second[:, portion * rows_second:(portion + 1) * rows_second], proj_second[portion * rows_second:(portion + 1) * rows_second], preferred_element_type=jnp.float32)
        rounded = lax.optimization_barrier(portion_sum.astype(jnp.bfloat16))
        mixture = mixture + rounded.astype(jnp.float32)
    residual = (residual_in.astype(jnp.float32) + mixture).astype(jnp.bfloat16)
    as_float = residual.astype(jnp.float32)
    inverse_rms = lax.rsqrt(lax.optimization_barrier(jnp.mean(as_float * as_float, axis=-1, keepdims=True)) + epsilon)
    normed = (as_float * inverse_rms * expert_norm.astype(jnp.float32)).astype(jnp.bfloat16)
    block_count = TOKENS // TOK_DEV
    owners, slot_ids = jax.vmap(route_tables)(route_ids.reshape(block_count, TOK_DEV, TOPK))
    slot_weight = jax.vmap(place_weights)(slot_ids, route_weight.reshape(block_count, TOK_DEV * TOPK))
    padded = jnp.concatenate((normed.reshape(block_count, TOK_DEV, D), jnp.zeros((block_count, 1, D), jnp.bfloat16)), axis=1)
    block_base = (jnp.arange(block_count, dtype=jnp.int32) * TOK_DEV).astype(jnp.int32)[:, None]
    quarter_width = FF // N_TP

    def expert_step(combined, inputs):
        gate_matrix, up_matrix, down_matrix, expert = inputs
        chosen = lax.dynamic_slice_in_dim(owners, (expert * CAP).astype(jnp.int32), CAP, 1)
        gathered = jax.vmap(pick_rows)(padded, chosen)
        flattened = gathered.reshape(block_count * CAP, D)
        gate_part = jnp.dot(flattened, gate_matrix, preferred_element_type=jnp.float32)
        up_part = jnp.dot(flattened, up_matrix, preferred_element_type=jnp.float32)
        hidden = (jax.nn.silu(gate_part) * up_part).astype(jnp.bfloat16)
        summed = jnp.zeros((block_count * CAP, D), jnp.float32)
        for portion in range(N_TP):
            piece = jnp.dot(hidden[:, portion * quarter_width:(portion + 1) * quarter_width], down_matrix[portion * quarter_width:(portion + 1) * quarter_width], preferred_element_type=jnp.float32)
            rounded = lax.optimization_barrier(piece.astype(jnp.bfloat16))
            summed = summed + rounded.astype(jnp.float32)
        weights_here = lax.dynamic_slice_in_dim(slot_weight, (expert * CAP).astype(jnp.int32), CAP, 1).reshape(-1, 1)
        targets = jnp.where(chosen == TOK_DEV, TOKENS, block_base + chosen).astype(jnp.int32).reshape(-1)
        combined = combined.at[targets].add(summed * weights_here)
        return (combined, None)
    combined_start = jnp.zeros((TOKENS + 1, D), jnp.float32)
    combined, _ = lax.scan(expert_step, combined_start, (expert_gate, expert_up, expert_down, jnp.arange(EXPERTS, dtype=jnp.int32)))
    return (residual.astype(jnp.float32) + combined[:TOKENS]).astype(jnp.bfloat16)
```

```python
import functools

import jax
import jax.numpy as jnp
from jax import lax
from jax.experimental import pallas as pl
from jax.experimental.pallas import tpu as pltpu
from jax.sharding import PartitionSpec as P

KA = 128
VA = 256
KB = 64
VB = 128
BLK = 64
PAIR = 2


epsilon = 1e-06
highest = lax.Precision.HIGHEST
MESH = pl.DeviceIdType.MESH
VMEM = pl.BlockSpec(memory_space=pltpu.VMEM)


def greet(peers):
    barrier = pltpu.get_barrier_semaphore()
    for peer in peers:
        pl.semaphore_signal(barrier, inc=1, device_id=peer, device_id_type=MESH)
    pl.semaphore_wait(barrier, len(peers))


def group_member(axis, span, step):
    me = lax.axis_index(axis)
    inside = lax.rem(me, span)
    other = lax.rem(inside + step, span)
    return inside, other, {axis: me - inside + other}


def exchange_kernel(axis, span, spread, count, *refs):
    sources, targets = refs[:count], refs[count : 2 * count]
    send_sems, recv_sems = refs[2 * count :]
    greet([group_member(axis, span, step)[2] for step in range(1, span)])
    copies = []
    for step in range(1, span):
        inside, other, device = group_member(axis, span, step)
        for i in range(count):
            copy = pltpu.make_async_remote_copy(
                src_ref=sources[i].at[other] if spread else sources[i],
                dst_ref=targets[i].at[inside],
                send_sem=send_sems.at[i, step],
                recv_sem=recv_sems.at[i, step],
                device_id=device,
                device_id_type=MESH,
            )
            copy.start()
            copies.append(copy)
    inside = lax.rem(lax.axis_index(axis), span)
    for i in range(count):
        targets[i][inside] = sources[i][inside] if spread else sources[i][...]
    for copy in copies:
        copy.wait()


def exchange(arrays, axis, span, spread, number):
    shapes = tuple(
        jax.ShapeDtypeStruct(a.shape if spread else (span,) + a.shape, a.dtype) for a in arrays
    )
    count = len(arrays)
    return pl.pallas_call(
        functools.partial(exchange_kernel, axis, span, spread, count),
        out_shape=shapes,
        in_specs=[VMEM] * count,
        out_specs=(VMEM,) * count,
        scratch_shapes=[
            pltpu.SemaphoreType.DMA((count, span)),
            pltpu.SemaphoreType.DMA((count, span)),
        ],
        compiler_params=pltpu.CompilerParams(collective_id=number, has_side_effects=True),
    )(*arrays)


def tp_member(across, sibling):
    size, me = lax.axis_size("tp"), lax.axis_index("tp")
    seat = lax.rem(me, PAIR)
    base = lax.rem(me - seat + across * PAIR, size)
    return base + (lax.rem(seat + 1, PAIR) if sibling else seat)


def remote(source, target, sems, index, device):
    return pltpu.make_async_remote_copy(
        src_ref=source,
        dst_ref=target,
        send_sem=sems[0].at[index],
        recv_sem=sems[1].at[index],
        device_id=device,
        device_id_type=MESH,
    )


def reduce_kernel(size, pairs, spread, source, target, near, paired, arrived, *rest):
    done = rest[0] if spread else None
    sems = rest[1:] if spread else rest
    pair_sems, far_sems, sp_sems = sems[:2], sems[2:4], sems[4:]
    me = lax.axis_index("sp")
    sibling = {"tp": tp_member(0, True)}
    far = [{"tp": tp_member(across, False)} for across in range(1, pairs)]
    peers = [group_member("sp", size, step) for step in range(1, size)] if spread else []
    greet([peer[2] for peer in peers] + [sibling] + far)
    order = [lax.rem(me + k + 1, size) if spread else k for k in range(size)]
    hops = list(range(1, pairs)) + [0]
    first = {}
    for k in range(size):
        for across in hops:
            copy = remote(
                source.at[tp_member(across, True), order[k]],
                near.at[across, order[k]],
                pair_sems,
                (across, k),
                sibling,
            )
            copy.start()
            first[k, across] = copy
    second = {}
    for k in range(size):
        for across in hops:
            first[k, across].wait_recv()
            total = source[tp_member(across, False), order[k]].astype(jnp.float32)
            total = total + near[across, order[k]].astype(jnp.float32)
            paired[across, order[k]] = total.astype(paired.dtype)
        for across in range(1, pairs):
            copy = remote(
                paired.at[across, order[k]],
                arrived.at[across, order[k]],
                far_sems,
                (across, k),
                far[across - 1],
            )
            copy.start()
            second[k, across] = copy
    third = []
    for k in range(size):
        total = paired[0, order[k]].astype(jnp.float32)
        for across in range(1, pairs):
            second[k, across].wait_recv()
            total = total + arrived[across, order[k]].astype(jnp.float32)
        if not spread:
            target[order[k]] = total
        elif k == size - 1:
            target[me] = total.astype(target.dtype)
        else:
            done[order[k]] = total.astype(done.dtype)
            copy = remote(done.at[order[k]], target.at[me], sp_sems, k, peers[k][2])
            copy.start()
            third.append(copy)
    for copy in list(first.values()) + list(second.values()):
        copy.wait_send()
    for copy in third:
        copy.wait()


def reduce_tp(blocks, spread, number):
    tp, size, rows, width = blocks.shape
    pairs = tp // PAIR
    kept = pltpu.VMEM((pairs, size, rows, width), jnp.bfloat16)
    done = [pltpu.VMEM((size, rows, width), jnp.bfloat16)] if spread else []
    return pl.pallas_call(
        functools.partial(reduce_kernel, size, pairs, spread),
        out_shape=jax.ShapeDtypeStruct(
            (size, rows, width), jnp.bfloat16 if spread else jnp.float32
        ),
        in_specs=[VMEM],
        out_specs=VMEM,
        scratch_shapes=[kept] * 3
        + done
        + [pltpu.SemaphoreType.DMA((pairs, size))] * 4
        + [pltpu.SemaphoreType.DMA((size,))] * 2,
        compiler_params=pltpu.CompilerParams(collective_id=number, has_side_effects=True),
    )(blocks)


def ring_offset(step, lines):
    return lax.rem(step * (lines // 2), lines) + step // 2


def experts_kernel(
    size,
    tp,
    slots_across,
    slots_down,
    route_weight,
    residual,
    gain,
    gate_hbm,
    up_hbm,
    down_hbm,
    out,
    gate_weights,
    up_weights,
    down_weights,
    chosen_rows,
    rows,
    normed,
    hidden,
    pieces,
    near,
    paired,
    arrived,
    done,
    returned,
    total,
    columns,
    collected,
    load_sems,
    *sems,
):
    out_sems, far_sems, pair_sems, near_sems, cross_sems, back_sems, last_sems = (
        sems[2 * i : 2 * i + 2] for i in range(7)
    )
    pairs = tp // PAIR
    lines = size // PAIR
    capacity, width = rows.shape[2:]
    tokens = residual.shape[0]
    me, mine = lax.axis_index("sp"), lax.axis_index("tp")
    line, seat = me // PAIR, lax.rem(me, PAIR)
    sibling = {"tp": tp_member(0, True)}

    def forth(k):
        across = lax.rem(line + ring_offset(k // PAIR, lines), lines)
        return across * PAIR + lax.rem(seat + lax.rem(k, PAIR), PAIR)

    def back(k):
        across = lax.rem(line - ring_offset(k // PAIR, lines) + lines, lines)
        return across * PAIR + lax.rem(seat + lax.rem(k, PAIR), PAIR)

    loads = [
        pltpu.make_async_copy(gate_hbm, gate_weights, load_sems.at[0]),
        pltpu.make_async_copy(up_hbm, up_weights, load_sems.at[1]),
        pltpu.make_async_copy(down_hbm, down_weights, load_sems.at[2]),
    ]
    for load in loads:
        load.start()
    peers = [group_member("sp", size, step)[2] for step in range(1, size)]
    peers += [group_member("tp", tp, step)[2] for step in range(1, tp)]
    greet(peers)

    def outward(k):
        return remote(
            chosen_rows.at[k], rows.at[me, mine], out_sems, k, {"sp": forth(k)}
        )

    def choose(k, target, *index):
        numbers = lax.broadcasted_iota(jnp.int32, (capacity, tokens), 0) + forth(k) * capacity
        chosen = numbers == slots_across[0:1, :]
        for c in range(1, slots_across.shape[0]):
            chosen = chosen | (numbers == slots_across[c : c + 1, :])
        picked = jnp.where(chosen, 1.0, 0.0).astype(jnp.bfloat16)
        picked = jnp.dot(picked, residual[...], preferred_element_type=jnp.float32)
        target[index] = picked.astype(jnp.bfloat16)

    choose(0, rows, me, mine)

    def send_step(k, carry):
        choose(k, chosen_rows, k)
        outward(k).start()
        return carry

    lax.fori_loop(1, size, send_step, 0)

    def to_far(k, across):
        block = rows.at[back(k), mine]
        return remote(block, block, far_sems, (across, k), {"tp": tp_member(across, False)})

    def to_pair(k, across):
        origin = tp_member(pairs - across, False) if across else mine
        block = rows.at[back(k), origin]
        return remote(block, block, pair_sems, (across, k), sibling)

    def forward(k):
        for across in range(1, pairs):
            to_far(k, across).start()
        to_pair(k, 0).start()

    def forward_group(g):
        for j in range(PAIR):
            k = g * PAIR + j
            outward(k).wait_recv()
            forward(k)

    def collect_group(g):
        for j in range(PAIR):
            for across in range(1, pairs):
                to_far(g * PAIR + j, across).wait_recv()
                to_pair(g * PAIR + j, across).start()
        for j in range(PAIR):
            for across in range(pairs):
                to_pair(g * PAIR + j, across).wait_recv()

    def to_near(g, across):
        return remote(
            pieces.at[g, tp_member(across, True)],
            near.at[g, across],
            near_sems,
            (across, g),
            sibling,
        )

    def to_cross(g, across):
        return remote(
            paired.at[g, across],
            arrived.at[g, across],
            cross_sems,
            (across, g),
            {"tp": tp_member(across, False)},
        )

    def homeward(k):
        return remote(
            done.at[k], returned.at[me], back_sems, k, {"sp": back(k)}
        )

    def run_group(g):
        for j in range(PAIR):
            origin = back(g * PAIR + j)
            block = jnp.concatenate([rows[origin, t] for t in range(tp)], axis=1)
            block = block.astype(jnp.float32)
            inverse = lax.rsqrt(jnp.mean(block * block, axis=1, keepdims=True) + epsilon)
            normed[j * capacity : (j + 1) * capacity] = (block * inverse * gain[...]).astype(
                jnp.bfloat16
            )
        gate_part = jnp.dot(normed[...], gate_weights[...], preferred_element_type=jnp.float32)
        up_part = jnp.dot(normed[...], up_weights[...], preferred_element_type=jnp.float32)
        hidden[...] = (jax.nn.silu(gate_part) * up_part).astype(jnp.bfloat16)
        for t in range(tp):
            piece = jnp.dot(
                hidden[...],
                down_weights[:, t * width : (t + 1) * width],
                preferred_element_type=jnp.float32,
            )
            pieces[g, t] = piece.astype(jnp.bfloat16)
        for across in list(range(1, pairs)) + [0]:
            to_near(g, across).start()

    def pair_sum(g, across):
        own = pieces[g, tp_member(across, False)].astype(jnp.float32)
        return own + near[g, across].astype(jnp.float32)

    def cross_group(g):
        for across in range(1, pairs):
            to_near(g, across).wait_recv()
            paired[g, across] = pair_sum(g, across).astype(jnp.bfloat16)
            to_cross(g, across).start()

    def finish_group(g, first):
        to_near(g, 0).wait_recv()
        summed = pair_sum(g, 0)
        for across in range(1, pairs):
            to_cross(g, across).wait_recv()
            summed = summed + arrived[g, across].astype(jnp.float32)
        summed = summed.astype(jnp.bfloat16)
        for j in range(PAIR):
            part = summed[j * capacity : (j + 1) * capacity]
            if first and j == 0:
                returned[me] = part
            else:
                done[g * PAIR + j] = part
                homeward(g * PAIR + j).start()

    forward(0)
    outward(1).wait_recv()
    forward(1)
    for load in loads:
        load.wait()
    groups = size // PAIR

    def group_step(g, carry):
        @pl.when(g + 1 < groups)
        def _():
            forward_group(g + 1)

        collect_group(g)
        run_group(g)

        @pl.when(g == 1)
        def _():
            finish_group(0, True)

        @pl.when(g > 1)
        def _():
            finish_group(g - 1, False)

        cross_group(g)
        return carry

    lax.fori_loop(0, groups, group_step, 0)
    finish_group(groups - 1, groups == 1)

    def combine(k):
        expert = forth(k)
        numbers = lax.broadcasted_iota(jnp.int32, (tokens, capacity), 1) + expert * capacity
        weights = jnp.zeros((tokens, capacity), jnp.float32)
        for c in range(route_weight.shape[1]):
            weights = weights + jnp.where(
                numbers == slots_down[:, c : c + 1], route_weight[:, c : c + 1], 0.0
            )
        coarse = weights.astype(jnp.bfloat16)
        fine = (weights - coarse.astype(jnp.float32)).astype(jnp.bfloat16)
        part = jnp.dot(coarse, returned[expert], preferred_element_type=jnp.float32)
        return part + jnp.dot(fine, returned[expert], preferred_element_type=jnp.float32)

    total[...] = residual[...].astype(jnp.float32) + combine(0)

    def combine_step(k, carry):
        homeward(k).wait_recv()
        total[...] += combine(k)
        return carry

    lax.fori_loop(1, size, combine_step, 0)
    own = tokens // tp
    for t in range(tp):
        columns[t] = total[t * own : (t + 1) * own].astype(jnp.bfloat16)

    def to_owner(step):
        _, other, device = group_member("tp", tp, step)
        return remote(columns.at[other], collected.at[mine], last_sems, step, device)

    for step in range(1, tp):
        to_owner(step).start()
    collected[mine] = columns[mine]
    for step in range(1, tp):
        to_owner(step).wait_recv()
    for t in range(tp):
        out[:, t * width : (t + 1) * width] = collected[t]

    def drain_step(k, carry):
        outward(k).wait_send()
        homeward(k).wait_send()
        return carry

    lax.fori_loop(1, size, drain_step, 0)

    def drain_pair(k, carry):
        for across in range(pairs):
            to_pair(k, across).wait_send()
            if across:
                to_far(k, across).wait_send()
        return carry

    lax.fori_loop(0, size, drain_pair, 0)

    def drain_group(g, carry):
        for across in range(pairs):
            to_near(g, across).wait_send()
            if across:
                to_cross(g, across).wait_send()
        return carry

    lax.fori_loop(0, groups, drain_group, 0)
    for step in range(1, tp):
        to_owner(step).wait_send()


def run_experts(slots, route_weight, residual, gain, gate, up, down, capacity, number):
    size, tp = lax.axis_size("sp"), lax.axis_size("tp")
    pairs, groups = tp // PAIR, size // PAIR
    tokens, width = residual.shape
    model, hidden = gate.shape
    half = jnp.bfloat16
    taken = PAIR * capacity
    anywhere = pl.BlockSpec(memory_space=pl.ANY)
    dma = pltpu.SemaphoreType.DMA
    return pl.pallas_call(
        functools.partial(experts_kernel, size, tp),
        out_shape=jax.ShapeDtypeStruct((tokens // tp, model), half),
        in_specs=[VMEM] * 5 + [anywhere] * 3,
        out_specs=VMEM,
        scratch_shapes=[
            pltpu.VMEM(gate.shape, half),
            pltpu.VMEM(up.shape, half),
            pltpu.VMEM(down.shape, half),
            pltpu.VMEM((size, capacity, width), half),
            pltpu.VMEM((size, tp, capacity, width), half),
            pltpu.VMEM((taken, model), half),
            pltpu.VMEM((taken, hidden), half),
            pltpu.VMEM((groups, tp, taken, width), half),
            pltpu.VMEM((groups, pairs, taken, width), half),
            pltpu.VMEM((groups, pairs, taken, width), half),
            pltpu.VMEM((groups, pairs, taken, width), half),
            pltpu.VMEM((size, capacity, width), half),
            pltpu.VMEM((size, capacity, width), half),
            pltpu.VMEM((tokens, width), jnp.float32),
            pltpu.VMEM((tp, tokens // tp, width), half),
            pltpu.VMEM((tp, tokens // tp, width), half),
            dma((3,)),
        ]
        + [dma((size,))] * 2
        + [dma((pairs, size))] * 4
        + [dma((pairs, groups))] * 4
        + [dma((size,))] * 2
        + [dma((tp,))] * 2,
        compiler_params=pltpu.CompilerParams(collective_id=number, has_side_effects=True),
    )(slots.T, slots, route_weight, residual, gain, gate, up, down)


def local_pass(queries, key_rows, values, decay_factors, key_width, value_width):
    count_of_tokens = queries.shape[0]
    head_count = queries.shape[1] // key_width
    blocks = count_of_tokens // BLK
    lower = jnp.tril(jnp.ones((BLK, BLK), jnp.float32))

    def arrange(source, feature_channels):
        return (
            source.astype(jnp.float32)
            .reshape(blocks, BLK, head_count, feature_channels)
            .transpose(0, 2, 1, 3)
        )

    query_blocks = arrange(queries, key_width) * key_width ** (-0.5)
    key_blocks = arrange(key_rows, key_width)
    value_blocks = arrange(values, value_width)
    cumulative = jnp.einsum("ts,nhsd->nhtd", lower, arrange(decay_factors, key_width), precision=highest)
    block_end = cumulative[:, :, -1:, :]
    query_decayed = query_blocks * jnp.exp(cumulative)
    key_inverse = key_blocks * jnp.exp(-cumulative)
    key_to_end = key_blocks * jnp.exp(block_end - cumulative)
    scores = jnp.einsum("nhtd,nhsd->nhts", query_decayed, key_inverse, precision=highest) * lower
    inner = jnp.einsum("nhts,nhsv->nhtv", scores, value_blocks, precision=highest)
    added = jnp.einsum("nhsd,nhsv->nhdv", key_to_end, value_blocks, precision=highest)
    state = jnp.zeros((head_count, key_width, value_width), jnp.float32)
    states = []
    for n in range(blocks):
        states.append(state)
        state = jnp.exp(block_end[n, :, 0])[:, :, None] * state + added[n]
    ends = block_end[:, :, 0]
    return (query_decayed, inner, jnp.stack(states), ends, state)


def finish_pass(query_decayed, inner, states, ends, entering):
    before = jnp.cumsum(ends, axis=0) - ends
    states = states + jnp.exp(before)[:, :, :, None] * entering[None]
    out = inner + jnp.einsum("nhtd,nhdv->nhtv", query_decayed, states, precision=highest)
    blocks, heads, rows, width = out.shape
    return out.transpose(0, 2, 1, 3).reshape(blocks * rows, heads, width)


def entering_state(totals, states, index):
    size = totals.shape[0]
    k = jnp.arange(size)
    reached = (k < index)[:, None]
    masked = jnp.where(reached, totals, 0.0)
    after = (k[None, :] > k[:, None]).astype(jnp.float32)
    behind = jnp.sum(after[:, :, None] * masked[None], axis=1)
    factor = jnp.where(reached, jnp.exp(behind), 0.0)
    return jnp.sum(factor[:, :, None] * states.astype(jnp.float32), axis=0)


def head_norm(attention, head_gain, gate):
    inverse_rms = lax.rsqrt(jnp.mean(attention * attention, axis=-1, keepdims=True) + epsilon)
    gate_silu = jax.nn.silu(gate.astype(jnp.float32).reshape(attention.shape))
    mixed_rows = attention * inverse_rms * head_gain * gate_silu
    return mixed_rows.astype(jnp.bfloat16).reshape(attention.shape[0], -1)


def route_positions(block_routes, experts):
    flattened = block_routes.reshape(-1)
    amount = flattened.shape[0]
    onehot = flattened[:, None] == jnp.arange(experts, dtype=jnp.int32)[None, :]
    earlier = jnp.tril(jnp.ones((amount, amount), jnp.bfloat16), -1)
    before = jnp.dot(earlier, onehot.astype(jnp.bfloat16), preferred_element_type=jnp.float32)
    ranking = jnp.sum(jnp.where(onehot, before, 0.0), axis=1).astype(jnp.int32)
    return ranking.reshape(block_routes.shape)


def shards(
    query_first,
    key_first,
    value_first,
    decay_first,
    gate_first,
    norm_first,
    proj_first,
    query_second,
    key_second,
    value_second,
    decay_second,
    gate_second,
    norm_second,
    proj_second,
    residual_in,
    expert_norm,
    route_ids,
    route_weight,
    expert_gate,
    expert_up,
    expert_down,
):
    sp_size, tp_size = lax.axis_size("sp"), lax.axis_size("tp")
    sp_index = lax.axis_index("sp")
    first = local_pass(query_first, key_first, value_first, decay_first, KA, VA)
    second = local_pass(query_second, key_second, value_second, decay_second, KB, VB)
    total_first = jnp.sum(first[3], axis=0).reshape(1, -1)
    total_second = jnp.sum(second[3], axis=0).reshape(1, -1)
    totals = jnp.concatenate((total_first, total_second), axis=1)
    totals = jnp.broadcast_to(totals, (8, totals.shape[1]))
    all_totals, all_first, all_second, *columns = exchange(
        (
            totals,
            first[4].reshape(-1, VA).astype(jnp.bfloat16),
            second[4].reshape(-1, VB).astype(jnp.bfloat16),
            proj_first,
            proj_second,
        ),
        "sp",
        sp_size,
        False,
        0,
    )
    columns = [part.transpose(1, 0, 2).reshape(part.shape[1], -1) for part in columns]
    projection = jnp.concatenate(columns, axis=0)
    cut = total_first.shape[1]
    enter_first = entering_state(all_totals[:, 0, :cut], all_first, sp_index)
    enter_second = entering_state(all_totals[:, 0, cut:], all_second, sp_index)
    attention_first = finish_pass(*first[:4], enter_first.reshape(first[4].shape))
    attention_second = finish_pass(*second[:4], enter_second.reshape(second[4].shape))
    mixed_first = head_norm(attention_first, norm_first, gate_first)
    mixed_second = head_norm(attention_second, norm_second, gate_second)
    mixed_rows = jnp.concatenate((mixed_first, mixed_second), axis=1)
    partial_terms = jnp.dot(mixed_rows, projection, preferred_element_type=jnp.float32)
    block_tokens, top_count = route_ids.shape
    model_width = partial_terms.shape[1]
    own_tokens = block_tokens // tp_size
    own_columns = model_width // tp_size
    by_owner = (block_tokens, tp_size, own_columns)
    partial_terms = partial_terms.astype(jnp.bfloat16).reshape(by_owner).transpose(1, 0, 2)
    partial_terms = partial_terms.reshape(tp_size, PAIR, block_tokens // PAIR, own_columns)
    mixture = reduce_tp(partial_terms, False, 1).reshape(block_tokens, own_columns)
    own_tokens = residual_in.shape[0]
    residual = residual_in.reshape(own_tokens, tp_size, own_columns).transpose(1, 0, 2)
    (residual,) = exchange((residual,), "tp", tp_size, True, 2)
    residual = residual.reshape(block_tokens, own_columns)
    residual = (residual.astype(jnp.float32) + mixture).astype(jnp.bfloat16)

    experts = sp_size
    capacity = 2 * top_count * block_tokens // experts
    slots = route_ids * capacity + route_positions(route_ids, experts)
    return run_experts(
        slots,
        route_weight,
        residual,
        expert_norm.reshape(1, -1),
        expert_gate[0],
        expert_up[0],
        expert_down[0],
        capacity,
        3,
    )


def solution(mesh):
    in_specs = (
        P("sp", "tp"),
        P("sp", "tp"),
        P("sp", "tp"),
        P("sp", "tp"),
        P("sp", "tp"),
        P(),
        P("tp", "sp"),
        P("sp", "tp"),
        P("sp", "tp"),
        P("sp", "tp"),
        P("sp", "tp"),
        P("sp", "tp"),
        P(),
        P("tp", "sp"),
        P(("sp", "tp"), None),
        P(),
        P("sp", None),
        P("sp", None),
        P("sp", None, "tp"),
        P("sp", None, "tp"),
        P("sp", "tp", None),
    )
    out_specs = P(("sp", "tp"), None)
    return jax.shard_map(shards, mesh=mesh, in_specs=in_specs, out_specs=out_specs, check_vma=False)
```

```python
import functools

import jax
import jax.numpy as jnp
from jax import lax
from jax.experimental import pallas as pl
from jax.experimental.pallas import tpu as pltpu
from jax.sharding import PartitionSpec as P

KA = 128
VA = 256
KB = 64
VB = 128
BLK = 64
PAIR = 2
LANES = 128


epsilon = 1e-06
highest = lax.Precision.HIGHEST
MESH = pl.DeviceIdType.MESH
VMEM = pl.BlockSpec(memory_space=pltpu.VMEM)


def greet(peers):
    barrier = pltpu.get_barrier_semaphore()
    for peer in peers:
        pl.semaphore_signal(barrier, inc=1, device_id=peer, device_id_type=MESH)
    pl.semaphore_wait(barrier, len(peers))


def group_member(axis, span, step):
    me = lax.axis_index(axis)
    inside = lax.rem(me, span)
    other = lax.rem(inside + step, span)
    return inside, other, {axis: me - inside + other}


def exchange_kernel(axis, span, spread, count, *refs):
    sources, targets = refs[:count], refs[count : 2 * count]
    send_sems, recv_sems = refs[2 * count :]
    greet([group_member(axis, span, step)[2] for step in range(1, span)])
    copies = []
    for step in range(1, span):
        inside, other, device = group_member(axis, span, step)
        for i in range(count):
            copy = pltpu.make_async_remote_copy(
                src_ref=sources[i].at[other] if spread else sources[i],
                dst_ref=targets[i].at[inside],
                send_sem=send_sems.at[i, step],
                recv_sem=recv_sems.at[i, step],
                device_id=device,
                device_id_type=MESH,
            )
            copy.start()
            copies.append(copy)
    inside = lax.rem(lax.axis_index(axis), span)
    for i in range(count):
        targets[i][inside] = sources[i][inside] if spread else sources[i][...]
    for copy in copies:
        copy.wait()


def exchange(arrays, axis, span, spread, number):
    shapes = tuple(
        jax.ShapeDtypeStruct(a.shape if spread else (span,) + a.shape, a.dtype) for a in arrays
    )
    count = len(arrays)
    return pl.pallas_call(
        functools.partial(exchange_kernel, axis, span, spread, count),
        out_shape=shapes,
        in_specs=[VMEM] * count,
        out_specs=(VMEM,) * count,
        scratch_shapes=[
            pltpu.SemaphoreType.DMA((count, span)),
            pltpu.SemaphoreType.DMA((count, span)),
        ],
        compiler_params=pltpu.CompilerParams(collective_id=number, has_side_effects=True),
    )(*arrays)


def tp_member(across, sibling):
    size, me = lax.axis_size("tp"), lax.axis_index("tp")
    seat = lax.rem(me, PAIR)
    base = lax.rem(me - seat + across * PAIR, size)
    return base + (lax.rem(seat + 1, PAIR) if sibling else seat)


def remote(source, target, sems, index, device):
    return pltpu.make_async_remote_copy(
        src_ref=source,
        dst_ref=target,
        send_sem=sems[0].at[index],
        recv_sem=sems[1].at[index],
        device_id=device,
        device_id_type=MESH,
    )


def reduce_kernel(size, pairs, spread, source, target, near, paired, arrived, *rest):
    done = rest[0] if spread else None
    sems = rest[1:] if spread else rest
    pair_sems, far_sems, sp_sems = sems[:2], sems[2:4], sems[4:]
    me = lax.axis_index("sp")
    sibling = {"tp": tp_member(0, True)}
    far = [{"tp": tp_member(across, False)} for across in range(1, pairs)]
    peers = [group_member("sp", size, step) for step in range(1, size)] if spread else []
    greet([peer[2] for peer in peers] + [sibling] + far)
    order = [lax.rem(me + k + 1, size) if spread else k for k in range(size)]
    hops = list(range(1, pairs)) + [0]
    first = {}
    for k in range(size):
        for across in hops:
            copy = remote(
                source.at[tp_member(across, True), order[k]],
                near.at[across, order[k]],
                pair_sems,
                (across, k),
                sibling,
            )
            copy.start()
            first[k, across] = copy
    second = {}
    for k in range(size):
        for across in hops:
            first[k, across].wait_recv()
            total = source[tp_member(across, False), order[k]].astype(jnp.float32)
            total = total + near[across, order[k]].astype(jnp.float32)
            paired[across, order[k]] = total.astype(paired.dtype)
        for across in range(1, pairs):
            copy = remote(
                paired.at[across, order[k]],
                arrived.at[across, order[k]],
                far_sems,
                (across, k),
                far[across - 1],
            )
            copy.start()
            second[k, across] = copy
    third = []
    for k in range(size):
        total = paired[0, order[k]].astype(jnp.float32)
        for across in range(1, pairs):
            second[k, across].wait_recv()
            total = total + arrived[across, order[k]].astype(jnp.float32)
        if not spread:
            target[order[k]] = total
        elif k == size - 1:
            target[me] = total.astype(target.dtype)
        else:
            done[order[k]] = total.astype(done.dtype)
            copy = remote(done.at[order[k]], target.at[me], sp_sems, k, peers[k][2])
            copy.start()
            third.append(copy)
    for copy in list(first.values()) + list(second.values()):
        copy.wait_send()
    for copy in third:
        copy.wait()


def reduce_tp(blocks, spread, number):
    tp, size, rows, width = blocks.shape
    pairs = tp // PAIR
    kept = pltpu.VMEM((pairs, size, rows, width), jnp.bfloat16)
    done = [pltpu.VMEM((size, rows, width), jnp.bfloat16)] if spread else []
    return pl.pallas_call(
        functools.partial(reduce_kernel, size, pairs, spread),
        out_shape=jax.ShapeDtypeStruct(
            (size, rows, width), jnp.bfloat16 if spread else jnp.float32
        ),
        in_specs=[VMEM],
        out_specs=VMEM,
        scratch_shapes=[kept] * 3
        + done
        + [pltpu.SemaphoreType.DMA((pairs, size))] * 4
        + [pltpu.SemaphoreType.DMA((size,))] * 2,
        compiler_params=pltpu.CompilerParams(collective_id=number, has_side_effects=True),
    )(blocks)


def ring_offset(step, lines):
    return lax.rem(step * (lines // 2), lines) + step // 2


def experts_kernel(
    size,
    tp,
    slots_across,
    slots_down,
    route_weight,
    residual,
    gain,
    gate_hbm,
    up_hbm,
    down_hbm,
    out,
    gate_weights,
    up_weights,
    down_weights,
    chosen_rows,
    rows,
    normed,
    hidden,
    pieces,
    near,
    paired,
    arrived,
    done,
    returned,
    total,
    columns,
    collected,
    load_sems,
    *sems,
):
    out_sems, far_sems, pair_sems, near_sems, cross_sems, back_sems, last_sems = (
        sems[2 * i : 2 * i + 2] for i in range(7)
    )
    pairs = tp // PAIR
    lines = size // PAIR
    capacity, width = rows.shape[2:]
    tokens = residual.shape[0]
    me, mine = lax.axis_index("sp"), lax.axis_index("tp")
    line, seat = me // PAIR, lax.rem(me, PAIR)
    sibling = {"tp": tp_member(0, True)}

    def forth(k):
        across = lax.rem(line + ring_offset(k // PAIR, lines), lines)
        return across * PAIR + lax.rem(seat + lax.rem(k, PAIR), PAIR)

    def back(k):
        across = lax.rem(line - ring_offset(k // PAIR, lines) + lines, lines)
        return across * PAIR + lax.rem(seat + lax.rem(k, PAIR), PAIR)

    loads = [
        pltpu.make_async_copy(gate_hbm, gate_weights, load_sems.at[0]),
        pltpu.make_async_copy(up_hbm, up_weights, load_sems.at[1]),
        pltpu.make_async_copy(down_hbm, down_weights, load_sems.at[2]),
    ]
    for load in loads:
        load.start()
    peers = [group_member("sp", size, step)[2] for step in range(1, size)]
    peers += [group_member("tp", tp, step)[2] for step in range(1, tp)]
    greet(peers)

    def outward(k):
        return remote(
            chosen_rows.at[k], rows.at[me, mine], out_sems, k, {"sp": forth(k)}
        )

    def choose(k, target, *index):
        numbers = lax.broadcasted_iota(jnp.int32, (capacity, tokens), 0) + forth(k) * capacity
        chosen = numbers == slots_across[0:1, :]
        for c in range(1, slots_across.shape[0]):
            chosen = chosen | (numbers == slots_across[c : c + 1, :])
        picked = jnp.where(chosen, 1.0, 0.0).astype(jnp.bfloat16)
        picked = jnp.dot(picked, residual[...], preferred_element_type=jnp.float32)
        target[index] = picked.astype(jnp.bfloat16)

    choose(0, rows, me, mine)

    def send_step(k, carry):
        choose(k, chosen_rows, k)
        outward(k).start()
        return carry

    lax.fori_loop(1, size, send_step, 0)

    def to_far(k, across):
        block = rows.at[back(k), mine]
        return remote(block, block, far_sems, (across, k), {"tp": tp_member(across, False)})

    def to_pair(k, across):
        origin = tp_member(pairs - across, False) if across else mine
        block = rows.at[back(k), origin]
        return remote(block, block, pair_sems, (across, k), sibling)

    def forward(k):
        for across in range(1, pairs):
            to_far(k, across).start()
        to_pair(k, 0).start()

    def forward_group(g):
        for j in range(PAIR):
            k = g * PAIR + j
            outward(k).wait_recv()
            forward(k)

    def collect_group(g):
        for j in range(PAIR):
            for across in range(1, pairs):
                to_far(g * PAIR + j, across).wait_recv()
                to_pair(g * PAIR + j, across).start()
        for j in range(PAIR):
            for across in range(pairs):
                to_pair(g * PAIR + j, across).wait_recv()

    def to_near(g, across):
        return remote(
            pieces.at[g, tp_member(across, True)],
            near.at[g, across],
            near_sems,
            (across, g),
            sibling,
        )

    def to_cross(g, across):
        return remote(
            paired.at[g, across],
            arrived.at[g, across],
            cross_sems,
            (across, g),
            {"tp": tp_member(across, False)},
        )

    def homeward(k):
        return remote(
            done.at[k], returned.at[me], back_sems, k, {"sp": back(k)}
        )

    def run_group(g):
        for j in range(PAIR):
            origin = back(g * PAIR + j)
            block = jnp.concatenate([rows[origin, t] for t in range(tp)], axis=1)
            block = block.astype(jnp.float32)
            inverse = lax.rsqrt(jnp.mean(block * block, axis=1, keepdims=True) + epsilon)
            normed[j * capacity : (j + 1) * capacity] = (block * inverse * gain[...]).astype(
                jnp.bfloat16
            )
        gate_part = jnp.dot(normed[...], gate_weights[...], preferred_element_type=jnp.float32)
        up_part = jnp.dot(normed[...], up_weights[...], preferred_element_type=jnp.float32)
        hidden[...] = (jax.nn.silu(gate_part) * up_part).astype(jnp.bfloat16)
        for t in range(tp):
            piece = jnp.dot(
                hidden[...],
                down_weights[:, t * width : (t + 1) * width],
                preferred_element_type=jnp.float32,
            )
            pieces[g, t] = piece.astype(jnp.bfloat16)
        for across in list(range(1, pairs)) + [0]:
            to_near(g, across).start()

    def pair_sum(g, across):
        own = pieces[g, tp_member(across, False)].astype(jnp.float32)
        return own + near[g, across].astype(jnp.float32)

    def cross_group(g):
        for across in range(1, pairs):
            to_near(g, across).wait_recv()
            paired[g, across] = pair_sum(g, across).astype(jnp.bfloat16)
            to_cross(g, across).start()

    def finish_group(g, first):
        to_near(g, 0).wait_recv()
        summed = pair_sum(g, 0)
        for across in range(1, pairs):
            to_cross(g, across).wait_recv()
            summed = summed + arrived[g, across].astype(jnp.float32)
        summed = summed.astype(jnp.bfloat16)
        for j in range(PAIR):
            part = summed[j * capacity : (j + 1) * capacity]
            if first and j == 0:
                returned[me] = part
            else:
                done[g * PAIR + j] = part
                homeward(g * PAIR + j).start()

    forward(0)
    outward(1).wait_recv()
    forward(1)
    for load in loads:
        load.wait()
    groups = size // PAIR

    def group_step(g, carry):
        @pl.when(g + 1 < groups)
        def _():
            forward_group(g + 1)

        collect_group(g)
        run_group(g)

        @pl.when(g == 1)
        def _():
            finish_group(0, True)

        @pl.when(g > 1)
        def _():
            finish_group(g - 1, False)

        cross_group(g)
        return carry

    lax.fori_loop(0, groups, group_step, 0)
    finish_group(groups - 1, groups == 1)

    def combine(k):
        expert = forth(k)
        numbers = lax.broadcasted_iota(jnp.int32, (tokens, capacity), 1) + expert * capacity
        weights = jnp.zeros((tokens, capacity), jnp.float32)
        for c in range(route_weight.shape[1]):
            weights = weights + jnp.where(
                numbers == slots_down[:, c : c + 1], route_weight[:, c : c + 1], 0.0
            )
        coarse = weights.astype(jnp.bfloat16)
        fine = (weights - coarse.astype(jnp.float32)).astype(jnp.bfloat16)
        part = jnp.dot(coarse, returned[expert], preferred_element_type=jnp.float32)
        return part + jnp.dot(fine, returned[expert], preferred_element_type=jnp.float32)

    total[...] = residual[...].astype(jnp.float32) + combine(0)

    def combine_step(k, carry):
        homeward(k).wait_recv()
        total[...] += combine(k)
        return carry

    lax.fori_loop(1, size, combine_step, 0)
    own = tokens // tp
    for t in range(tp):
        columns[t] = total[t * own : (t + 1) * own].astype(jnp.bfloat16)

    def to_owner(step):
        _, other, device = group_member("tp", tp, step)
        return remote(columns.at[other], collected.at[mine], last_sems, step, device)

    for step in range(1, tp):
        to_owner(step).start()
    collected[mine] = columns[mine]
    for step in range(1, tp):
        to_owner(step).wait_recv()
    for t in range(tp):
        out[:, t * width : (t + 1) * width] = collected[t]

    def drain_step(k, carry):
        outward(k).wait_send()
        homeward(k).wait_send()
        return carry

    lax.fori_loop(1, size, drain_step, 0)

    def drain_pair(k, carry):
        for across in range(pairs):
            to_pair(k, across).wait_send()
            if across:
                to_far(k, across).wait_send()
        return carry

    lax.fori_loop(0, size, drain_pair, 0)

    def drain_group(g, carry):
        for across in range(pairs):
            to_near(g, across).wait_send()
            if across:
                to_cross(g, across).wait_send()
        return carry

    lax.fori_loop(0, groups, drain_group, 0)
    for step in range(1, tp):
        to_owner(step).wait_send()


def run_experts(slots, route_weight, residual, gain, gate, up, down, capacity, number):
    size, tp = lax.axis_size("sp"), lax.axis_size("tp")
    pairs, groups = tp // PAIR, size // PAIR
    tokens, width = residual.shape
    model, hidden = gate.shape
    half = jnp.bfloat16
    taken = PAIR * capacity
    anywhere = pl.BlockSpec(memory_space=pl.ANY)
    dma = pltpu.SemaphoreType.DMA
    return pl.pallas_call(
        functools.partial(experts_kernel, size, tp),
        out_shape=jax.ShapeDtypeStruct((tokens // tp, model), half),
        in_specs=[VMEM] * 5 + [anywhere] * 3,
        out_specs=VMEM,
        scratch_shapes=[
            pltpu.VMEM(gate.shape, half),
            pltpu.VMEM(up.shape, half),
            pltpu.VMEM(down.shape, half),
            pltpu.VMEM((size, capacity, width), half),
            pltpu.VMEM((size, tp, capacity, width), half),
            pltpu.VMEM((taken, model), half),
            pltpu.VMEM((taken, hidden), half),
            pltpu.VMEM((groups, tp, taken, width), half),
            pltpu.VMEM((groups, pairs, taken, width), half),
            pltpu.VMEM((groups, pairs, taken, width), half),
            pltpu.VMEM((groups, pairs, taken, width), half),
            pltpu.VMEM((size, capacity, width), half),
            pltpu.VMEM((size, capacity, width), half),
            pltpu.VMEM((tokens, width), jnp.float32),
            pltpu.VMEM((tp, tokens // tp, width), half),
            pltpu.VMEM((tp, tokens // tp, width), half),
            dma((3,)),
        ]
        + [dma((size,))] * 2
        + [dma((pairs, size))] * 4
        + [dma((pairs, groups))] * 4
        + [dma((size,))] * 2
        + [dma((tp,))] * 2,
        compiler_params=pltpu.CompilerParams(collective_id=number, has_side_effects=True),
    )(slots.T, slots, route_weight, residual, gain, gate, up, down)


def halves(value):
    coarse = value.astype(jnp.bfloat16)
    return coarse, (value - coarse.astype(jnp.float32)).astype(jnp.bfloat16)


def contract(left, right, left_axis, right_axis):
    return lax.dot_general(
        left,
        right,
        (((left_axis,), (right_axis,)), ((), ())),
        preferred_element_type=jnp.float32,
    )


def rows_by_rows(left, right):
    (a, b), (c, d) = halves(left), halves(right)
    return contract(a, c, 1, 1) + (contract(a, d, 1, 1) + contract(b, c, 1, 1))


def mixer_kernel(size, tp, *refs):
    (query_first, key_first, value_first, decay_first, gate_first, norm_first, proj_first) = refs[:7]
    (query_second, key_second, value_second, decay_second) = refs[7:11]
    (gate_second, norm_second, proj_second, residual_in, out) = refs[11:16]
    (projection, attended, early, state, state_sent, state_near, total_sent, total_near) = refs[16:24]
    (carry_in, carry_out, entering, mixed, part, near, paired, arrived, given, taken) = refs[24:34]
    sems = refs[34:]
    recv_sems, up_sems, down_sems, side_sems = sems[:4]
    state_sems, total_sems, carry_sems, near_sems, cross_sems, row_sems = (
        sems[4 + 2 * i : 6 + 2 * i] for i in range(6)
    )
    pairs, lines, share = tp // PAIR, size // PAIR, size // tp
    tokens = query_first.shape[0]
    blocks = tokens // BLK
    wide_first, wide_second = query_first.shape[1], query_second.shape[1]
    deep_first, deep_second = value_first.shape[1], value_second.shape[1]
    cuts = projection.shape[1]
    height = projection.shape[2]
    width = part.shape[2]
    me, mine = lax.axis_index("sp"), lax.axis_index("tp")
    line, seat = me // PAIR, lax.rem(me, PAIR)
    sibling = {"tp": tp_member(0, True)}
    side = {"sp": line * PAIR + lax.rem(seat + 1, PAIR)}
    above = {"sp": lax.rem(line + 1, lines) * PAIR + seat}
    below = {"sp": lax.rem(line + lines - 1, lines) * PAIR + seat}
    greet([side, above, below] + [group_member("tp", tp, step)[2] for step in range(1, tp)])
    has_above, has_below = line + 1 < lines, line > 0

    def own_piece(p):
        half = cuts // 2
        source = proj_first if p < half else proj_second
        return source.at[pl.ds((p % half) * height, height)]

    def hop(source, chunk, p, send_sems, device):
        return pltpu.make_async_remote_copy(
            src_ref=source,
            dst_ref=projection.at[chunk, p],
            send_sem=send_sems.at[chunk, p],
            recv_sem=recv_sems.at[chunk, p],
            device_id=device,
            device_id_type=MESH,
        )

    def relay(chunk, p, send_sems, device):
        return hop(projection.at[chunk, p], chunk, p, send_sems, device)

    for p in range(cuts):

        @pl.when(has_above)
        def _():
            hop(own_piece(p), me, p, up_sems, above).start()

        @pl.when(has_below)
        def _():
            hop(own_piece(p), me, p, down_sems, below).start()

        if p < cuts // 2:
            hop(own_piece(p), me, p, side_sems, side).start()

    own_rows, own_width = taken.shape[1:]
    for t in range(tp):
        given[t] = residual_in[:, t * own_width : (t + 1) * own_width]

    def to_owner(step):
        _, other, device = group_member("tp", tp, step)
        return remote(given.at[other], taken.at[mine], row_sems, step, device)

    for step in range(1, tp):
        to_owner(step).start()
    taken[mine] = given[mine]

    earlier = lax.broadcasted_iota(jnp.int32, (tokens, tokens), 0)
    later = lax.broadcasted_iota(jnp.int32, (tokens, tokens), 1)
    causal = (earlier >= later) & (earlier // BLK == later // BLK)
    lower = jnp.where(causal, 1.0, 0.0).astype(jnp.bfloat16)
    decay = jnp.concatenate([decay_first[...], decay_second[...]], axis=1)
    high, low = halves(decay)
    rest = (decay - high.astype(jnp.float32) - low.astype(jnp.float32)).astype(jnp.bfloat16)
    running = contract(lower, high, 1, 0) + (contract(lower, low, 1, 0) + contract(lower, rest, 1, 0))
    ends = [running[(n + 1) * BLK - 1 : (n + 1) * BLK] for n in range(blocks)]
    before = [jnp.zeros_like(ends[0])]
    for n in range(blocks):
        before.append(before[n] + ends[n])

    def spread(parts):
        shape = (BLK, decay.shape[1])
        return jnp.concatenate([jnp.broadcast_to(part_row, shape) for part_row in parts], axis=0)

    queries = jnp.concatenate(
        [
            query_first[...].astype(jnp.float32) * KA ** (-0.5),
            query_second[...].astype(jnp.float32) * KB ** (-0.5),
        ],
        axis=1,
    )
    keys = jnp.concatenate([key_first[...], key_second[...]], axis=1).astype(jnp.float32)
    decayed = queries * jnp.exp(running)
    inverse = keys * jnp.exp(-running)
    to_end = keys * jnp.exp(spread(ends) - running)
    entry = decayed * jnp.exp(spread(before[:blocks]))
    early[...] = entry
    lanes = lax.broadcasted_iota(jnp.int32, (1, LANES), 1)

    heads = []
    for h in range(wide_first // KA):
        heads.append((h * KA, None, value_first, h * VA, VA, h * VA, h * VA))
    for h in range(wide_second // KB):
        base, inside = h * KB // LANES, h % (LANES // KB)
        heads.append(
            (
                wide_first + base * LANES,
                inside,
                value_second,
                h * VB,
                VB,
                deep_first + base * VB,
                deep_first + h * VB,
            )
        )

    def keep(value, inside):
        if inside is None:
            return value
        return jnp.where(lanes // KB == inside, value, 0.0)

    for lane, inside, values, column, depth, _, target in heads:
        scores = rows_by_rows(
            keep(decayed[:, lane : lane + LANES], inside), inverse[:, lane : lane + LANES]
        )
        a, b = halves(jnp.where(causal, scores, 0.0))
        value = values[:, column : column + depth]
        attended[:, target : target + depth] = contract(a, value, 1, 0) + contract(b, value, 1, 0)

    state[...] = jnp.zeros_like(state)
    for n in range(blocks):
        span = slice(n * BLK, (n + 1) * BLK)
        if n:
            for lane, inside, _, _, depth, row, target in heads:
                attended[span, target : target + depth] += rows_by_rows(
                    keep(decayed[span, lane : lane + LANES], inside), state[row : row + depth]
                )
        done = set()
        for lane, inside, values, column, depth, row, _ in heads:
            a, b = halves(to_end[span, lane : lane + LANES])
            value = values[span, column : column + depth]
            added = keep(contract(value, a, 0, 0) + contract(value, b, 0, 0), inside)
            if row not in done:
                done.add(row)
                added = added + state[row : row + depth] * jnp.exp(ends[n][:, lane : lane + LANES])
                state[row : row + depth] = added
            else:
                state[row : row + depth] += added

    state_sent[...] = state[...].astype(jnp.bfloat16)
    total_sent[...] = jnp.broadcast_to(before[blocks], total_sent.shape)
    swap_state = remote(state_sent, state_near, state_sems, 0, side)
    swap_total = remote(total_sent, total_near, total_sems, 0, side)
    swap_total.start()
    swap_state.start()
    for p in range(cuts // 2, cuts):
        hop(own_piece(p), me, p, side_sems, side).start()
    for p in range(cuts):
        projection[me, p] = own_piece(p)[...]

    def faded(total, row, depth, value):
        lane = row // VA * LANES if row < deep_first else wide_first + (row - deep_first) // VB * LANES
        return value * jnp.exp(total[:, lane : lane + LANES])

    portions = [(row, VB) for row in range(0, state.shape[0], VB)]

    def carry(i):
        row, depth = portions[i]
        return remote(
            carry_out.at[pl.ds(row, depth)], carry_in.at[pl.ds(row, depth)], carry_sems, i, above
        )

    def chain():
        swap_total.wait_recv()
        swap_state.wait_recv()
        own_total, other_total = total_sent[0:1, :], total_near[0:1, :]

        @pl.when(line == 0)
        def _():
            carry_in[...] = jnp.zeros_like(carry_in)

        lead = (seat == 0).astype(jnp.float32)
        total_lead = lead * own_total + (1.0 - lead) * other_total
        total_last = lead * other_total + (1.0 - lead) * own_total
        for i, (row, depth) in enumerate(portions):

            @pl.when(has_below)
            def _():
                carry(i).wait_recv()

            span = slice(row, row + depth)
            own, other = state[span], state_near[span].astype(jnp.float32)
            state_lead = lead * own + (1.0 - lead) * other
            state_last = lead * other + (1.0 - lead) * own
            come = carry_in[span].astype(jnp.float32)
            middle = faded(total_lead, row, depth, come) + state_lead
            carry_out[span] = (faded(total_last, row, depth, middle) + state_last).astype(jnp.bfloat16)

            @pl.when(has_above)
            def _():
                carry(i).start()

            entering[span] = lead * come + (1.0 - lead) * middle

    def pass_on(d, c):
        lower_chunk = jnp.maximum(line - d, 0) * PAIR + seat
        upper_chunk = jnp.minimum(line + d, lines - 1) * PAIR + seat
        for p in range(cuts):

            @pl.when(line >= d)
            def _():
                hop(projection.at[lower_chunk, p], lower_chunk, p, up_sems, above).wait_recv()

                @pl.when(has_above)
                def _():
                    relay(lower_chunk, p, up_sems, above).start()

                relay(lower_chunk, p, side_sems, side).start()

            @pl.when(line + d < lines)
            def _():
                relay(upper_chunk, p, down_sems, below).wait_recv()

                @pl.when(has_below)
                def _():
                    relay(upper_chunk, p, down_sems, below).start()

                relay(upper_chunk, p, side_sems, side).start()

        @pl.when(d == jnp.clip(line, 1, max(lines - 2, 1)))
        def _():
            chain()

        return c

    lax.fori_loop(1, lines, pass_on, 0)

    for lane, inside, _, _, depth, row, target in heads:
        span = slice(target, target + depth)
        attention = attended[:, span] + rows_by_rows(
            keep(early[:, lane : lane + LANES], inside), entering[row : row + depth]
        )
        first = target < deep_first
        gates = gate_first[:, span] if first else gate_second[:, target - deep_first : target - deep_first + depth]
        gates = gates.astype(jnp.float32)
        gain = norm_first[...] if first else norm_second[...]
        scale = lax.rsqrt(jnp.mean(attention * attention, axis=1, keepdims=True) + epsilon)
        mixed[:, span] = (attention * scale * gain * jax.nn.silu(gates)).astype(jnp.bfloat16)

    def arrive(i, c):
        chunk = i * PAIR + lax.rem(seat + 1, PAIR)
        for p in range(cuts):
            relay(chunk, p, side_sems, side).wait_recv()
        return c

    lax.fori_loop(0, lines, arrive, 0)

    def project(owner):
        for i in range(share):
            chunk = owner * share + i
            partial_sum = jnp.zeros((tokens, width), jnp.float32)
            for p in range(cuts):
                partial_sum = partial_sum + jnp.dot(
                    mixed[:, p * height : (p + 1) * height],
                    projection[chunk, p],
                    preferred_element_type=jnp.float32,
                )
            part[chunk] = partial_sum.astype(jnp.bfloat16)

    def to_near(across):
        return remote(
            part.at[pl.ds(tp_member(across, True) * share, share)],
            near.at[across],
            near_sems,
            across,
            sibling,
        )

    def to_cross(across):
        return remote(
            paired.at[across],
            arrived.at[across],
            cross_sems,
            across,
            {"tp": tp_member(across, False)},
        )

    hops = list(range(1, pairs)) + [0]
    for across in hops:
        project(tp_member(across, True))
        to_near(across).start()
        project(tp_member(across, False))
        if across:
            to_near(across).wait_recv()
            for i in range(share):
                summed = part[tp_member(across, False) * share + i].astype(jnp.float32)
                paired[across, i] = (summed + near[across, i].astype(jnp.float32)).astype(jnp.bfloat16)
            to_cross(across).start()
    for step in range(1, tp):
        to_owner(step).wait_recv()
    to_near(0).wait_recv()
    for across in range(1, pairs):
        to_cross(across).wait_recv()
    for i in range(share):
        summed = part[mine * share + i].astype(jnp.float32) + near[0, i].astype(jnp.float32)
        for across in range(1, pairs):
            summed = summed + arrived[across, i].astype(jnp.float32)
        for t in range(tp):
            base = taken[t, :, i * width : (i + 1) * width].astype(jnp.float32)
            rows = slice(t * own_rows, (t + 1) * own_rows)
            out[rows, i * width : (i + 1) * width] = (base + summed[rows]).astype(jnp.bfloat16)

    swap_state.wait_send()
    swap_total.wait_send()
    for i in range(len(portions)):

        @pl.when(has_above)
        def _():
            carry(i).wait_send()

    def drain(i, c):
        chunk = i * PAIR + seat
        for p in range(cuts):
            relay(chunk, p, side_sems, side).wait_send()

            @pl.when(has_above & (i <= line))
            def _():
                relay(chunk, p, up_sems, above).wait_send()

            @pl.when(has_below & (i >= line))
            def _():
                relay(chunk, p, down_sems, below).wait_send()

        return c

    lax.fori_loop(0, lines, drain, 0)
    for across in range(pairs):
        to_near(across).wait_send()
        if across:
            to_cross(across).wait_send()
    for step in range(1, tp):
        to_owner(step).wait_send()


def run_mixer(first, second, residual_in, number):
    size, tp = lax.axis_size("sp"), lax.axis_size("tp")
    pairs, share = tp // PAIR, size // tp
    tokens = first[0].shape[0]
    rows, width = first[-1].shape
    cuts = 4
    height = 2 * rows // cuts
    depth = first[2].shape[1] + second[2].shape[1]
    keys = first[0].shape[1] + second[0].shape[1]
    kept = first[2].shape[1] + second[0].shape[1] // LANES * VB
    own_rows, model = residual_in.shape
    half, single, dma = jnp.bfloat16, jnp.float32, pltpu.SemaphoreType.DMA
    return pl.pallas_call(
        functools.partial(mixer_kernel, size, tp),
        out_shape=jax.ShapeDtypeStruct((tokens, model // tp), half),
        in_specs=[VMEM] * 15,
        out_specs=VMEM,
        scratch_shapes=[
            pltpu.VMEM((size, cuts, height, width), half),
            pltpu.VMEM((tokens, depth), single),
            pltpu.VMEM((tokens, keys), single),
            pltpu.VMEM((kept, LANES), single),
            pltpu.VMEM((kept, LANES), half),
            pltpu.VMEM((kept, LANES), half),
            pltpu.VMEM((8, keys), single),
            pltpu.VMEM((8, keys), single),
            pltpu.VMEM((kept, LANES), half),
            pltpu.VMEM((kept, LANES), half),
            pltpu.VMEM((kept, LANES), single),
            pltpu.VMEM((tokens, depth), half),
            pltpu.VMEM((size, tokens, width), half),
            pltpu.VMEM((pairs, share, tokens, width), half),
            pltpu.VMEM((pairs, share, tokens, width), half),
            pltpu.VMEM((pairs, share, tokens, width), half),
            pltpu.VMEM((tp, own_rows, model // tp), half),
            pltpu.VMEM((tp, own_rows, model // tp), half),
        ]
        + [dma((size, cuts))] * 4
        + [dma((1,))] * 4
        + [dma((kept // VB,))] * 2
        + [dma((pairs,))] * 4
        + [dma((tp,))] * 2,
        compiler_params=pltpu.CompilerParams(collective_id=number, has_side_effects=True),
    )(*first, *second, residual_in)


def local_pass(queries, key_rows, values, decay_factors, key_width, value_width):
    count_of_tokens = queries.shape[0]
    head_count = queries.shape[1] // key_width
    blocks = count_of_tokens // BLK
    lower = jnp.tril(jnp.ones((BLK, BLK), jnp.float32))

    def arrange(source, feature_channels):
        return (
            source.astype(jnp.float32)
            .reshape(blocks, BLK, head_count, feature_channels)
            .transpose(0, 2, 1, 3)
        )

    query_blocks = arrange(queries, key_width) * key_width ** (-0.5)
    key_blocks = arrange(key_rows, key_width)
    value_blocks = arrange(values, value_width)
    cumulative = jnp.einsum("ts,nhsd->nhtd", lower, arrange(decay_factors, key_width), precision=highest)
    block_end = cumulative[:, :, -1:, :]
    query_decayed = query_blocks * jnp.exp(cumulative)
    key_inverse = key_blocks * jnp.exp(-cumulative)
    key_to_end = key_blocks * jnp.exp(block_end - cumulative)
    scores = jnp.einsum("nhtd,nhsd->nhts", query_decayed, key_inverse, precision=highest) * lower
    inner = jnp.einsum("nhts,nhsv->nhtv", scores, value_blocks, precision=highest)
    added = jnp.einsum("nhsd,nhsv->nhdv", key_to_end, value_blocks, precision=highest)
    state = jnp.zeros((head_count, key_width, value_width), jnp.float32)
    states = []
    for n in range(blocks):
        states.append(state)
        state = jnp.exp(block_end[n, :, 0])[:, :, None] * state + added[n]
    ends = block_end[:, :, 0]
    return (query_decayed, inner, jnp.stack(states), ends, state)


def finish_pass(query_decayed, inner, states, ends, entering):
    before = jnp.cumsum(ends, axis=0) - ends
    states = states + jnp.exp(before)[:, :, :, None] * entering[None]
    out = inner + jnp.einsum("nhtd,nhdv->nhtv", query_decayed, states, precision=highest)
    blocks, heads, rows, width = out.shape
    return out.transpose(0, 2, 1, 3).reshape(blocks * rows, heads, width)


def entering_state(totals, states, index):
    size = totals.shape[0]
    k = jnp.arange(size)
    reached = (k < index)[:, None]
    masked = jnp.where(reached, totals, 0.0)
    after = (k[None, :] > k[:, None]).astype(jnp.float32)
    behind = jnp.sum(after[:, :, None] * masked[None], axis=1)
    factor = jnp.where(reached, jnp.exp(behind), 0.0)
    return jnp.sum(factor[:, :, None] * states.astype(jnp.float32), axis=0)


def head_norm(attention, head_gain, gate):
    inverse_rms = lax.rsqrt(jnp.mean(attention * attention, axis=-1, keepdims=True) + epsilon)
    gate_silu = jax.nn.silu(gate.astype(jnp.float32).reshape(attention.shape))
    mixed_rows = attention * inverse_rms * head_gain * gate_silu
    return mixed_rows.astype(jnp.bfloat16).reshape(attention.shape[0], -1)


def route_positions(block_routes, experts):
    flattened = block_routes.reshape(-1)
    amount = flattened.shape[0]
    onehot = flattened[:, None] == jnp.arange(experts, dtype=jnp.int32)[None, :]
    earlier = jnp.tril(jnp.ones((amount, amount), jnp.bfloat16), -1)
    before = jnp.dot(earlier, onehot.astype(jnp.bfloat16), preferred_element_type=jnp.float32)
    ranking = jnp.sum(jnp.where(onehot, before, 0.0), axis=1).astype(jnp.int32)
    return ranking.reshape(block_routes.shape)


def plain_mixer(first, second, residual_in):
    query_first, key_first, value_first, decay_first, gate_first, norm_first, proj_first = first
    query_second, key_second, value_second, decay_second = second[:4]
    gate_second, norm_second, proj_second = second[4:]
    sp_size, tp_size = lax.axis_size("sp"), lax.axis_size("tp")
    sp_index = lax.axis_index("sp")
    here = local_pass(query_first, key_first, value_first, decay_first, KA, VA)
    there = local_pass(query_second, key_second, value_second, decay_second, KB, VB)
    total_first = jnp.sum(here[3], axis=0).reshape(1, -1)
    total_second = jnp.sum(there[3], axis=0).reshape(1, -1)
    totals = jnp.concatenate((total_first, total_second), axis=1)
    totals = jnp.broadcast_to(totals, (8, totals.shape[1]))
    all_totals, all_first, all_second, *columns = exchange(
        (
            totals,
            here[4].reshape(-1, VA).astype(jnp.bfloat16),
            there[4].reshape(-1, VB).astype(jnp.bfloat16),
            proj_first,
            proj_second,
        ),
        "sp",
        sp_size,
        False,
        0,
    )
    columns = [part.transpose(1, 0, 2).reshape(part.shape[1], -1) for part in columns]
    projection = jnp.concatenate(columns, axis=0)
    cut = total_first.shape[1]
    enter_first = entering_state(all_totals[:, 0, :cut], all_first, sp_index)
    enter_second = entering_state(all_totals[:, 0, cut:], all_second, sp_index)
    attention_first = finish_pass(*here[:4], enter_first.reshape(here[4].shape))
    attention_second = finish_pass(*there[:4], enter_second.reshape(there[4].shape))
    mixed_first = head_norm(attention_first, norm_first, gate_first)
    mixed_second = head_norm(attention_second, norm_second, gate_second)
    mixed_rows = jnp.concatenate((mixed_first, mixed_second), axis=1)
    partial_terms = jnp.dot(mixed_rows, projection, preferred_element_type=jnp.float32)
    block_tokens = query_first.shape[0]
    model_width = partial_terms.shape[1]
    own_tokens = block_tokens // tp_size
    own_columns = model_width // tp_size
    by_owner = (block_tokens, tp_size, own_columns)
    partial_terms = partial_terms.astype(jnp.bfloat16).reshape(by_owner).transpose(1, 0, 2)
    partial_terms = partial_terms.reshape(tp_size, PAIR, block_tokens // PAIR, own_columns)
    mixture = reduce_tp(partial_terms, False, 1).reshape(block_tokens, own_columns)
    own_tokens = residual_in.shape[0]
    residual = residual_in.reshape(own_tokens, tp_size, own_columns).transpose(1, 0, 2)
    (residual,) = exchange((residual,), "tp", tp_size, True, 2)
    residual = residual.reshape(block_tokens, own_columns)
    return (residual.astype(jnp.float32) + mixture).astype(jnp.bfloat16)


def shards(
    query_first,
    key_first,
    value_first,
    decay_first,
    gate_first,
    norm_first,
    proj_first,
    query_second,
    key_second,
    value_second,
    decay_second,
    gate_second,
    norm_second,
    proj_second,
    residual_in,
    expert_norm,
    route_ids,
    route_weight,
    expert_gate,
    expert_up,
    expert_down,
):
    sp_size, tp_size = lax.axis_size("sp"), lax.axis_size("tp")
    first = (query_first, key_first, value_first, decay_first, gate_first)
    first += (norm_first.reshape(1, -1), proj_first)
    second = (query_second, key_second, value_second, decay_second, gate_second)
    second += (norm_second.reshape(1, -1), proj_second)
    whole_lanes = proj_first.shape[1] % LANES == 0 and query_second.shape[1] % LANES == 0
    if whole_lanes and proj_first.shape == proj_second.shape and sp_size % tp_size == 0:
        residual = run_mixer(first, second, residual_in, 0)
    else:
        residual = plain_mixer(first, second, residual_in)
    block_tokens, top_count = route_ids.shape
    experts = sp_size
    capacity = 2 * top_count * block_tokens // experts
    slots = route_ids * capacity + route_positions(route_ids, experts)
    return run_experts(
        slots,
        route_weight,
        residual,
        expert_norm.reshape(1, -1),
        expert_gate[0],
        expert_up[0],
        expert_down[0],
        capacity,
        3,
    )


def solution(mesh):
    in_specs = (
        P("sp", "tp"),
        P("sp", "tp"),
        P("sp", "tp"),
        P("sp", "tp"),
        P("sp", "tp"),
        P(),
        P("tp", "sp"),
        P("sp", "tp"),
        P("sp", "tp"),
        P("sp", "tp"),
        P("sp", "tp"),
        P("sp", "tp"),
        P(),
        P("tp", "sp"),
        P(("sp", "tp"), None),
        P(),
        P("sp", None),
        P("sp", None),
        P("sp", None, "tp"),
        P("sp", None, "tp"),
        P("sp", "tp", None),
    )
    out_specs = P(("sp", "tp"), None)
    return jax.shard_map(shards, mesh=mesh, in_specs=in_specs, out_specs=out_specs, check_vma=False)
```

```python
import functools

import jax
import jax.numpy as jnp
from jax import lax
from jax.experimental import pallas as pl
from jax.experimental.pallas import tpu as pltpu
from jax.sharding import PartitionSpec as P

KA = 128
VA = 256
KB = 64
VB = 128
BLK = 64
PAIR = 2
LANES = 128


epsilon = 1e-06
highest = lax.Precision.HIGHEST
MESH = pl.DeviceIdType.MESH
VMEM = pl.BlockSpec(memory_space=pltpu.VMEM)


def greet(peers):
    barrier = pltpu.get_barrier_semaphore()
    for peer in peers:
        pl.semaphore_signal(barrier, inc=1, device_id=peer, device_id_type=MESH)
    pl.semaphore_wait(barrier, len(peers))


def group_member(axis, span, step):
    me = lax.axis_index(axis)
    inside = lax.rem(me, span)
    other = lax.rem(inside + step, span)
    return inside, other, {axis: me - inside + other}


def exchange_kernel(axis, span, spread, count, *refs):
    sources, targets = refs[:count], refs[count : 2 * count]
    send_sems, recv_sems = refs[2 * count :]
    greet([group_member(axis, span, step)[2] for step in range(1, span)])
    copies = []
    for step in range(1, span):
        inside, other, device = group_member(axis, span, step)
        for i in range(count):
            copy = pltpu.make_async_remote_copy(
                src_ref=sources[i].at[other] if spread else sources[i],
                dst_ref=targets[i].at[inside],
                send_sem=send_sems.at[i, step],
                recv_sem=recv_sems.at[i, step],
                device_id=device,
                device_id_type=MESH,
            )
            copy.start()
            copies.append(copy)
    inside = lax.rem(lax.axis_index(axis), span)
    for i in range(count):
        targets[i][inside] = sources[i][inside] if spread else sources[i][...]
    for copy in copies:
        copy.wait()


def exchange(arrays, axis, span, spread, number):
    shapes = tuple(
        jax.ShapeDtypeStruct(a.shape if spread else (span,) + a.shape, a.dtype) for a in arrays
    )
    count = len(arrays)
    return pl.pallas_call(
        functools.partial(exchange_kernel, axis, span, spread, count),
        out_shape=shapes,
        in_specs=[VMEM] * count,
        out_specs=(VMEM,) * count,
        scratch_shapes=[
            pltpu.SemaphoreType.DMA((count, span)),
            pltpu.SemaphoreType.DMA((count, span)),
        ],
        compiler_params=pltpu.CompilerParams(collective_id=number, has_side_effects=True),
    )(*arrays)


def tp_member(across, sibling):
    size, me = lax.axis_size("tp"), lax.axis_index("tp")
    seat = lax.rem(me, PAIR)
    base = lax.rem(me - seat + across * PAIR, size)
    return base + (lax.rem(seat + 1, PAIR) if sibling else seat)


def remote(source, target, sems, index, device):
    return pltpu.make_async_remote_copy(
        src_ref=source,
        dst_ref=target,
        send_sem=sems[0].at[index],
        recv_sem=sems[1].at[index],
        device_id=device,
        device_id_type=MESH,
    )


def reduce_kernel(size, pairs, spread, source, target, near, paired, arrived, *rest):
    done = rest[0] if spread else None
    sems = rest[1:] if spread else rest
    pair_sems, far_sems, sp_sems = sems[:2], sems[2:4], sems[4:]
    me = lax.axis_index("sp")
    sibling = {"tp": tp_member(0, True)}
    far = [{"tp": tp_member(across, False)} for across in range(1, pairs)]
    peers = [group_member("sp", size, step) for step in range(1, size)] if spread else []
    greet([peer[2] for peer in peers] + [sibling] + far)
    order = [lax.rem(me + k + 1, size) if spread else k for k in range(size)]
    hops = list(range(1, pairs)) + [0]
    first = {}
    for k in range(size):
        for across in hops:
            copy = remote(
                source.at[tp_member(across, True), order[k]],
                near.at[across, order[k]],
                pair_sems,
                (across, k),
                sibling,
            )
            copy.start()
            first[k, across] = copy
    second = {}
    for k in range(size):
        for across in hops:
            first[k, across].wait_recv()
            total = source[tp_member(across, False), order[k]].astype(jnp.float32)
            total = total + near[across, order[k]].astype(jnp.float32)
            paired[across, order[k]] = total.astype(paired.dtype)
        for across in range(1, pairs):
            copy = remote(
                paired.at[across, order[k]],
                arrived.at[across, order[k]],
                far_sems,
                (across, k),
                far[across - 1],
            )
            copy.start()
            second[k, across] = copy
    third = []
    for k in range(size):
        total = paired[0, order[k]].astype(jnp.float32)
        for across in range(1, pairs):
            second[k, across].wait_recv()
            total = total + arrived[across, order[k]].astype(jnp.float32)
        if not spread:
            target[order[k]] = total
        elif k == size - 1:
            target[me] = total.astype(target.dtype)
        else:
            done[order[k]] = total.astype(done.dtype)
            copy = remote(done.at[order[k]], target.at[me], sp_sems, k, peers[k][2])
            copy.start()
            third.append(copy)
    for copy in list(first.values()) + list(second.values()):
        copy.wait_send()
    for copy in third:
        copy.wait()


def reduce_tp(blocks, spread, number):
    tp, size, rows, width = blocks.shape
    pairs = tp // PAIR
    kept = pltpu.VMEM((pairs, size, rows, width), jnp.bfloat16)
    done = [pltpu.VMEM((size, rows, width), jnp.bfloat16)] if spread else []
    return pl.pallas_call(
        functools.partial(reduce_kernel, size, pairs, spread),
        out_shape=jax.ShapeDtypeStruct(
            (size, rows, width), jnp.bfloat16 if spread else jnp.float32
        ),
        in_specs=[VMEM],
        out_specs=VMEM,
        scratch_shapes=[kept] * 3
        + done
        + [pltpu.SemaphoreType.DMA((pairs, size))] * 4
        + [pltpu.SemaphoreType.DMA((size,))] * 2,
        compiler_params=pltpu.CompilerParams(collective_id=number, has_side_effects=True),
    )(blocks)


def experts_kernel(
    size,
    tp,
    unit,
    route_ids,
    route_weight,
    residual,
    gain,
    gate_hbm,
    up_hbm,
    down_hbm,
    collected,
    gate_weights,
    up_weights,
    down_weights,
    chosen_rows,
    rows,
    normed,
    hidden,
    pieces,
    near,
    paired,
    arrived,
    done,
    returned,
    total,
    columns,
    slots_across,
    load_sems,
    *sems,
):
    out_sems, far_sems, pair_sems, near_sems, cross_sems, back_sems, last_sems = (
        sems[2 * i : 2 * i + 2] for i in range(7)
    )
    pairs = tp // PAIR
    lines = size // PAIR
    capacity, width = rows.shape[2:]
    tokens = residual.shape[0]
    me, mine = lax.axis_index("sp"), lax.axis_index("tp")
    line, seat = me // PAIR, lax.rem(me, PAIR)
    sibling = {"tp": tp_member(0, True)}

    def partner(k):
        turn = k // PAIR
        turn = jnp.where(turn > 0, lax.rem(turn, max(lines - 1, 1)) + 1, 0)
        across = mirrored(line, turn, lines)
        return across * PAIR + lax.rem(seat + lax.rem(k, PAIR), PAIR)

    loads = [
        pltpu.make_async_copy(gate_hbm, gate_weights, load_sems.at[0]),
        pltpu.make_async_copy(up_hbm, up_weights, load_sems.at[1]),
        pltpu.make_async_copy(down_hbm, down_weights, load_sems.at[2]),
    ]
    for load in loads:
        load.start()
    numbers = lax.broadcasted_iota(jnp.int32, (size, tokens), 0)
    hits = [numbers == route_ids[c : c + 1, :] for c in range(route_ids.shape[0])]
    named = sum(jnp.where(hit, 1.0, 0.0) for hit in hits).astype(jnp.bfloat16)
    shape = (tokens, tokens)
    prior = lax.broadcasted_iota(jnp.int32, shape, 0) < lax.broadcasted_iota(jnp.int32, shape, 1)
    prior = jnp.where(prior, 1.0, 0.0).astype(jnp.bfloat16)
    counts = jnp.dot(named, prior, preferred_element_type=jnp.float32)
    for c, hit in enumerate(hits):
        rank = jnp.sum(jnp.where(hit, counts, 0.0), axis=0, keepdims=True).astype(jnp.int32)
        slots_across[c : c + 1, :] = route_ids[c : c + 1, :] * capacity + rank
    peers = [group_member("sp", size, step)[2] for step in range(1, size)]
    peers += [group_member("tp", tp, step)[2] for step in range(1, tp)]
    greet(peers)

    def outward(k):
        return remote(
            chosen_rows.at[k], rows.at[me, mine], out_sems, k, {"sp": partner(k)}
        )

    def choose(k, target, *index):
        numbers = lax.broadcasted_iota(jnp.int32, (capacity, tokens), 0) + partner(k) * capacity
        chosen = numbers == slots_across[0:1, :]
        for c in range(1, slots_across.shape[0]):
            chosen = chosen | (numbers == slots_across[c : c + 1, :])
        picked = jnp.where(chosen, 1.0, 0.0).astype(jnp.bfloat16)
        picked = jnp.dot(picked, residual[...], preferred_element_type=jnp.float32)
        target[index] = picked.astype(jnp.bfloat16)

    choose(0, rows, me, mine)

    def send_step(i, carry):
        last = i + size - 2 * PAIR
        k = jnp.where(i < PAIR, i, jnp.where(i < 2 * PAIR, last, i - PAIR))
        choose(k, chosen_rows, k)
        outward(k).start()
        return carry

    lax.fori_loop(1, size, send_step, 0)

    def to_far(k, across):
        block = rows.at[partner(k), mine]
        return remote(block, block, far_sems, (across, k), {"tp": tp_member(across, False)})

    def to_pair(k, across):
        origin = tp_member(pairs - across, False) if across else mine
        block = rows.at[partner(k), origin]
        return remote(block, block, pair_sems, (across, k), sibling)

    def forward(k):
        for across in range(1, pairs):
            to_far(k, across).start()
        to_pair(k, 0).start()

    def forward_group(g):
        for j in range(unit):
            k = g * unit + j
            outward(k).wait_recv()
            forward(k)

    def collect_group(g):
        for j in range(unit):
            for across in range(1, pairs):
                to_far(g * unit + j, across).wait_recv()
                to_pair(g * unit + j, across).start()
        for j in range(unit):
            for across in range(pairs):
                to_pair(g * unit + j, across).wait_recv()

    def to_near(g, across):
        return remote(
            pieces.at[g, tp_member(across, True)],
            near.at[g, across],
            near_sems,
            (across, g),
            sibling,
        )

    def to_cross(g, across):
        return remote(
            paired.at[g, across],
            arrived.at[g, across],
            cross_sems,
            (across, g),
            {"tp": tp_member(across, False)},
        )

    def homeward(k):
        return remote(
            done.at[k], returned.at[me], back_sems, k, {"sp": partner(k)}
        )

    def run_group(g):
        for j in range(unit):
            origin = partner(g * unit + j)
            block = jnp.concatenate([rows[origin, t] for t in range(tp)], axis=1)
            block = block.astype(jnp.float32)
            inverse = lax.rsqrt(jnp.mean(block * block, axis=1, keepdims=True) + epsilon)
            normed[j * capacity : (j + 1) * capacity] = (block * inverse * gain[...]).astype(
                jnp.bfloat16
            )
        gate_part = jnp.dot(normed[...], gate_weights[...], preferred_element_type=jnp.float32)
        up_part = jnp.dot(normed[...], up_weights[...], preferred_element_type=jnp.float32)
        hidden[...] = (jax.nn.silu(gate_part) * up_part).astype(jnp.bfloat16)
        for t in range(tp):
            piece = jnp.dot(
                hidden[...],
                down_weights[:, t * width : (t + 1) * width],
                preferred_element_type=jnp.float32,
            )
            pieces[g, t] = piece.astype(jnp.bfloat16)
        for across in list(range(1, pairs)) + [0]:
            to_near(g, across).start()

    def pair_sum(g, across):
        own = pieces[g, tp_member(across, False)].astype(jnp.float32)
        return own + near[g, across].astype(jnp.float32)

    def cross_group(g):
        for across in range(1, pairs):
            to_near(g, across).wait_recv()
            paired[g, across] = pair_sum(g, across).astype(jnp.bfloat16)
            to_cross(g, across).start()

    def finish_group(g, first):
        to_near(g, 0).wait_recv()
        summed = pair_sum(g, 0)
        for across in range(1, pairs):
            to_cross(g, across).wait_recv()
            summed = summed + arrived[g, across].astype(jnp.float32)
        summed = summed.astype(jnp.bfloat16)
        for j in range(unit):
            part = summed[j * capacity : (j + 1) * capacity]
            if first and j == 0:
                returned[me] = part
            else:
                done[g * unit + j] = part
                homeward(g * unit + j).start()

    forward(0)
    for k in range(1, unit):
        outward(k).wait_recv()
        forward(k)
    for load in loads:
        load.wait()
    groups = size // unit

    def group_step(g, carry):
        @pl.when(g + 1 < groups)
        def _():
            forward_group(g + 1)

        collect_group(g)
        run_group(g)

        cross_group(g)

        @pl.when(g == 1)
        def _():
            finish_group(0, True)

        @pl.when(g > 1)
        def _():
            finish_group(g - 1, False)

        return carry

    lax.fori_loop(0, groups, group_step, 0)
    finish_group(groups - 1, groups == 1)

    def combine(k):
        expert = partner(k)
        numbers = lax.broadcasted_iota(jnp.int32, (capacity, tokens), 0) + expert * capacity
        weights = jnp.zeros((capacity, tokens), jnp.float32)
        for c in range(route_weight.shape[0]):
            weights = weights + jnp.where(
                numbers == slots_across[c : c + 1, :], route_weight[c : c + 1, :], 0.0
            )
        coarse, fine = halves(weights)
        part = contract(coarse, returned[expert], 0, 0)
        return part + contract(fine, returned[expert], 0, 0)

    total[...] = residual[...].astype(jnp.float32) + combine(0)

    def combine_step(k, carry):
        homeward(k).wait_recv()
        total[...] += combine(k)
        return carry

    lax.fori_loop(1, size, combine_step, 0)
    own = tokens // tp
    for t in range(tp):
        columns[t] = total[t * own : (t + 1) * own].astype(jnp.bfloat16)

    def to_owner(step):
        _, other, device = group_member("tp", tp, step)
        return remote(columns.at[other], collected.at[mine], last_sems, step, device)

    for step in range(1, tp):
        to_owner(step).start()
    collected[mine] = columns[mine]
    for step in range(1, tp):
        to_owner(step).wait_recv()

    def drain_step(k, carry):
        outward(k).wait_send()
        homeward(k).wait_send()
        return carry

    lax.fori_loop(1, size, drain_step, 0)

    def drain_pair(k, carry):
        for across in range(pairs):
            to_pair(k, across).wait_send()
            if across:
                to_far(k, across).wait_send()
        return carry

    lax.fori_loop(0, size, drain_pair, 0)

    def drain_group(g, carry):
        for across in range(pairs):
            to_near(g, across).wait_send()
            if across:
                to_cross(g, across).wait_send()
        return carry

    lax.fori_loop(0, groups, drain_group, 0)
    for step in range(1, tp):
        to_owner(step).wait_send()


def run_experts(route_ids, route_weight, residual, gain, gate, up, down, capacity, number):
    size, tp = lax.axis_size("sp"), lax.axis_size("tp")
    unit = 1
    pairs, groups = tp // PAIR, size // unit
    tokens, width = residual.shape
    model, hidden = gate.shape
    half = jnp.bfloat16
    taken = unit * capacity
    anywhere = pl.BlockSpec(memory_space=pl.ANY)
    dma = pltpu.SemaphoreType.DMA
    collected = pl.pallas_call(
        functools.partial(experts_kernel, size, tp, unit),
        out_shape=jax.ShapeDtypeStruct((tp, tokens // tp, width), half),
        in_specs=[VMEM] * 4 + [anywhere] * 3,
        out_specs=VMEM,
        scratch_shapes=[
            pltpu.VMEM(gate.shape, half),
            pltpu.VMEM(up.shape, half),
            pltpu.VMEM(down.shape, half),
            pltpu.VMEM((size, capacity, width), half),
            pltpu.VMEM((size, tp, capacity, width), half),
            pltpu.VMEM((taken, model), half),
            pltpu.VMEM((taken, hidden), half),
            pltpu.VMEM((groups, tp, taken, width), half),
            pltpu.VMEM((groups, pairs, taken, width), half),
            pltpu.VMEM((groups, pairs, taken, width), half),
            pltpu.VMEM((groups, pairs, taken, width), half),
            pltpu.VMEM((size, capacity, width), half),
            pltpu.VMEM((size, capacity, width), half),
            pltpu.VMEM((tokens, width), jnp.float32),
            pltpu.VMEM((tp, tokens // tp, width), half),
            pltpu.VMEM(route_ids.shape[::-1], jnp.int32),
            dma((3,)),
        ]
        + [dma((size,))] * 2
        + [dma((pairs, size))] * 4
        + [dma((pairs, groups))] * 4
        + [dma((size,))] * 2
        + [dma((tp,))] * 2,
        compiler_params=pltpu.CompilerParams(collective_id=number, has_side_effects=True),
    )(route_ids.T, route_weight.T, residual, gain, gate, up, down)
    return collected.transpose(1, 0, 2).reshape(tokens // tp, model)


def mirrored(line, step, lines):
    if lines & (lines - 1):
        return lax.rem(step + lines - line, lines)
    place, bit = 0, 1
    while bit < lines:
        place = place + lax.rem(line // bit + step // bit, 2) * bit
        bit = 2 * bit
    return place


def halves(value):
    coarse = value.astype(jnp.bfloat16)
    return coarse, (value - coarse.astype(jnp.float32)).astype(jnp.bfloat16)


def contract(left, right, left_axis, right_axis):
    return lax.dot_general(
        left,
        right,
        (((left_axis,), (right_axis,)), ((), ())),
        preferred_element_type=jnp.float32,
    )


def rows_by_rows(left, right):
    (a, b), (c, d) = halves(left), halves(right)
    return contract(a, c, 1, 1) + (contract(a, d, 1, 1) + contract(b, c, 1, 1))


def mixer_kernel(size, tp, *refs):
    (query_first, key_first, value_first, decay_first, gate_first, norm_first, proj_first) = refs[:7]
    (query_second, key_second, value_second, decay_second) = refs[7:11]
    (gate_second, norm_second, proj_second, residual_in, out) = refs[11:16]
    (projection, attended, early, state, state_sent, state_near, total_sent, total_near) = refs[16:24]
    (carry_in, carry_out, entering, mixed, part, near, paired, arrived, given, taken) = refs[24:34]
    sems = refs[34:]
    recv_sems, up_sems, down_sems, side_sems = sems[:4]
    state_sems, total_sems, carry_sems, near_sems, cross_sems, row_sems = (
        sems[4 + 2 * i : 6 + 2 * i] for i in range(6)
    )
    pairs, lines, share = tp // PAIR, size // PAIR, size // tp
    tokens = query_first.shape[0]
    blocks = tokens // BLK
    wide_first, wide_second = query_first.shape[1], query_second.shape[1]
    deep_first, deep_second = value_first.shape[1], value_second.shape[1]
    cuts = projection.shape[1]
    height = projection.shape[2]
    width = part.shape[2]
    me, mine = lax.axis_index("sp"), lax.axis_index("tp")
    line, seat = me // PAIR, lax.rem(me, PAIR)
    sibling = {"tp": tp_member(0, True)}
    side = {"sp": line * PAIR + lax.rem(seat + 1, PAIR)}
    above = {"sp": lax.rem(line + 1, lines) * PAIR + seat}
    below = {"sp": lax.rem(line + lines - 1, lines) * PAIR + seat}
    greet([side, above, below] + [group_member("tp", tp, step)[2] for step in range(1, tp)])
    has_above, has_below = line + 1 < lines, line > 0

    def own_piece(p):
        half = cuts // 2
        source = proj_first if p < half else proj_second
        return source.at[pl.ds((p % half) * height, height)]

    def hop(source, chunk, p, send_sems, device):
        return pltpu.make_async_remote_copy(
            src_ref=source,
            dst_ref=projection.at[chunk, p],
            send_sem=send_sems.at[chunk, p],
            recv_sem=recv_sems.at[chunk, p],
            device_id=device,
            device_id_type=MESH,
        )

    def relay(chunk, p, send_sems, device):
        return hop(projection.at[chunk, p], chunk, p, send_sems, device)

    for p in range(cuts):

        @pl.when(has_above)
        def _():
            hop(own_piece(p), me, p, up_sems, above).start()

        @pl.when(has_below)
        def _():
            hop(own_piece(p), me, p, down_sems, below).start()

    crossed = cuts - 1
    for p in (crossed, 0):
        hop(own_piece(p), me, p, side_sems, side).start()
    own_rows, own_width = taken.shape[1:]
    for t in range(tp):
        given[t] = residual_in[:, t * own_width : (t + 1) * own_width]

    def to_owner(step):
        _, other, device = group_member("tp", tp, step)
        return remote(given.at[other], taken.at[mine], row_sems, step, device)

    for step in range(1, tp):
        to_owner(step).start()
    taken[mine] = given[mine]

    earlier = lax.broadcasted_iota(jnp.int32, (tokens, tokens), 0)
    later = lax.broadcasted_iota(jnp.int32, (tokens, tokens), 1)
    causal = (earlier >= later) & (earlier // BLK == later // BLK)
    lower = jnp.where(causal, 1.0, 0.0).astype(jnp.bfloat16)
    decay = jnp.concatenate([decay_first[...], decay_second[...]], axis=1)
    high, low = halves(decay)
    rest = (decay - high.astype(jnp.float32) - low.astype(jnp.float32)).astype(jnp.bfloat16)
    running = contract(lower, high, 1, 0) + (contract(lower, low, 1, 0) + contract(lower, rest, 1, 0))
    ends = [running[(n + 1) * BLK - 1 : (n + 1) * BLK] for n in range(blocks)]
    before = [jnp.zeros_like(ends[0])]
    for n in range(blocks):
        before.append(before[n] + ends[n])

    def spread(parts):
        shape = (BLK, decay.shape[1])
        return jnp.concatenate([jnp.broadcast_to(part_row, shape) for part_row in parts], axis=0)

    queries = jnp.concatenate(
        [
            query_first[...].astype(jnp.float32) * KA ** (-0.5),
            query_second[...].astype(jnp.float32) * KB ** (-0.5),
        ],
        axis=1,
    )
    keys = jnp.concatenate([key_first[...], key_second[...]], axis=1).astype(jnp.float32)
    decayed = queries * jnp.exp(running)
    inverse = keys * jnp.exp(-running)
    to_end = keys * jnp.exp(spread(ends) - running)
    entry = decayed * jnp.exp(spread(before[:blocks]))
    early[...] = entry
    lanes = lax.broadcasted_iota(jnp.int32, (1, LANES), 1)

    heads = []
    for h in range(wide_first // KA):
        heads.append((h * KA, None, value_first, h * VA, VA, h * VA, h * VA))
    for h in range(wide_second // KB):
        base, inside = h * KB // LANES, h % (LANES // KB)
        heads.append(
            (
                wide_first + base * LANES,
                inside,
                value_second,
                h * VB,
                VB,
                deep_first + base * VB,
                deep_first + h * VB,
            )
        )

    def keep(value, inside):
        if inside is None:
            return value
        return jnp.where(lanes // KB == inside, value, 0.0)

    for lane, inside, values, column, depth, _, target in heads:
        scores = rows_by_rows(
            keep(decayed[:, lane : lane + LANES], inside), inverse[:, lane : lane + LANES]
        )
        a, b = halves(jnp.where(causal, scores, 0.0))
        value = values[:, column : column + depth]
        attended[:, target : target + depth] = contract(a, value, 1, 0) + contract(b, value, 1, 0)

    state[...] = jnp.zeros_like(state)
    for n in range(blocks):
        span = slice(n * BLK, (n + 1) * BLK)
        if n:
            for lane, inside, _, _, depth, row, target in heads:
                attended[span, target : target + depth] += rows_by_rows(
                    keep(decayed[span, lane : lane + LANES], inside), state[row : row + depth]
                )
        done = set()
        for lane, inside, values, column, depth, row, _ in heads:
            a, b = halves(to_end[span, lane : lane + LANES])
            value = values[span, column : column + depth]
            added = keep(contract(value, a, 0, 0) + contract(value, b, 0, 0), inside)
            if row not in done:
                done.add(row)
                added = added + state[row : row + depth] * jnp.exp(ends[n][:, lane : lane + LANES])
                state[row : row + depth] = added
            else:
                state[row : row + depth] += added

    state_sent[...] = state[...].astype(jnp.bfloat16)
    total_sent[...] = jnp.broadcast_to(before[blocks], total_sent.shape)
    swap_state = remote(state_sent, state_near, state_sems, 0, side)
    swap_total = remote(total_sent, total_near, total_sems, 0, side)
    swap_total.start()
    swap_state.start()
    for p in range(1, crossed):
        hop(own_piece(p), me, p, side_sems, side).start()
    beside = line * PAIR + lax.rem(seat + 1, PAIR)
    relay(beside, crossed, side_sems, side).wait_recv()

    @pl.when(has_above)
    def _():
        relay(beside, crossed, up_sems, above).start()

    @pl.when(has_below)
    def _():
        relay(beside, crossed, down_sems, below).start()

    for p in range(cuts):
        projection[me, p] = own_piece(p)[...]

    def faded(total, row, depth, value):
        lane = row // VA * LANES if row < deep_first else wide_first + (row - deep_first) // VB * LANES
        return value * jnp.exp(total[:, lane : lane + LANES])

    portions = [(row, VB) for row in range(0, state.shape[0], VB)]

    def carry(i):
        row, depth = portions[i]
        return remote(
            carry_out.at[pl.ds(row, depth)], carry_in.at[pl.ds(row, depth)], carry_sems, i, above
        )

    def chain():
        swap_total.wait_recv()
        swap_state.wait_recv()
        own_total, other_total = total_sent[0:1, :], total_near[0:1, :]

        @pl.when(line == 0)
        def _():
            carry_in[...] = jnp.zeros_like(carry_in)

        lead = (seat == 0).astype(jnp.float32)
        total_lead = lead * own_total + (1.0 - lead) * other_total
        total_last = lead * other_total + (1.0 - lead) * own_total
        for i, (row, depth) in enumerate(portions):

            @pl.when(has_below)
            def _():
                carry(i).wait_recv()

            span = slice(row, row + depth)
            own, other = state[span], state_near[span].astype(jnp.float32)
            state_lead = lead * own + (1.0 - lead) * other
            state_last = lead * other + (1.0 - lead) * own
            come = carry_in[span].astype(jnp.float32)
            middle = faded(total_lead, row, depth, come) + state_lead
            carry_out[span] = (faded(total_last, row, depth, middle) + state_last).astype(jnp.bfloat16)

            @pl.when(has_above)
            def _():
                carry(i).start()

            entering[span] = lead * come + (1.0 - lead) * middle

    def pass_on(d, c):
        lower_line = jnp.maximum(line - d, 0) * PAIR
        upper_line = jnp.minimum(line + d, lines - 1) * PAIR
        for p in range(cuts):
            for other in range(PAIR if p == crossed else 1):
                place = lax.rem(seat + other, PAIR)
                lower_chunk, upper_chunk = lower_line + place, upper_line + place

                @pl.when(line >= d)
                def _():
                    relay(lower_chunk, p, up_sems, above).wait_recv()

                    @pl.when(has_above)
                    def _():
                        relay(lower_chunk, p, up_sems, above).start()

                    if p != crossed:
                        relay(lower_chunk, p, side_sems, side).start()

                @pl.when(line + d < lines)
                def _():
                    relay(upper_chunk, p, down_sems, below).wait_recv()

                    @pl.when(has_below)
                    def _():
                        relay(upper_chunk, p, down_sems, below).start()

                    if p != crossed:
                        relay(upper_chunk, p, side_sems, side).start()

        @pl.when(d == jnp.clip(line, 1, max(lines - 2, 1)))
        def _():
            chain()

        return c

    lax.fori_loop(1, lines, pass_on, 0)

    for lane, inside, _, _, depth, row, target in heads:
        span = slice(target, target + depth)
        attention = attended[:, span] + rows_by_rows(
            keep(early[:, lane : lane + LANES], inside), entering[row : row + depth]
        )
        first = target < deep_first
        gates = gate_first[:, span] if first else gate_second[:, target - deep_first : target - deep_first + depth]
        gates = gates.astype(jnp.float32)
        gain = norm_first[...] if first else norm_second[...]
        scale = lax.rsqrt(jnp.mean(attention * attention, axis=1, keepdims=True) + epsilon)
        mixed[:, span] = (attention * scale * gain * jax.nn.silu(gates)).astype(jnp.bfloat16)

    def project(owner):
        for i in range(share):
            chunk = owner * share + i
            partial_sum = jnp.zeros((tokens, width), jnp.float32)
            for p in range(cuts):
                partial_sum = partial_sum + jnp.dot(
                    mixed[:, p * height : (p + 1) * height],
                    projection[chunk, p],
                    preferred_element_type=jnp.float32,
                )
            part[chunk] = partial_sum.astype(jnp.bfloat16)

    def to_near(across):
        return remote(
            part.at[pl.ds(tp_member(across, True) * share, share)],
            near.at[across],
            near_sems,
            across,
            sibling,
        )

    def to_cross(across):
        return remote(
            paired.at[across],
            arrived.at[across],
            cross_sems,
            across,
            {"tp": tp_member(across, False)},
        )

    tp_seat = lax.rem(mine, PAIR)

    def across_of(owner):
        return lax.rem(owner // PAIR - mine // PAIR + pairs, pairs)

    def begin(owner):
        chunk = owner * PAIR + lax.rem(seat + 1, PAIR)
        for p in range(crossed):
            relay(chunk, p, side_sems, side).wait_recv()
        project(owner)

        @pl.when(lax.rem(owner, PAIR) != tp_seat)
        def _():
            to_near(across_of(owner)).start()

    def settle(owner):
        across = across_of(owner)

        @pl.when((lax.rem(owner, PAIR) == tp_seat) & (across > 0))
        def _():
            to_near(across).wait_recv()
            for i in range(share):
                summed = part[owner * share + i].astype(jnp.float32)
                paired[across, i] = (summed + near[across, i].astype(jnp.float32)).astype(jnp.bfloat16)
            to_cross(across).start()

    inner = (line > 0) & (line + 1 < lines)
    owners = []
    for i in range(tp):
        place = mirrored(line, i, lines)
        if 2 <= i and lines == 4:
            place = jnp.where(inner, mirrored(line, 5 - i, lines), place)
        owners.append(place)
    for i in range(tp):
        begin(owners[i])
        if i:
            settle(owners[i - 1])
    settle(owners[tp - 1])
    for step in range(1, tp):
        to_owner(step).wait_recv()
    to_near(0).wait_recv()
    for across in range(1, pairs):
        to_cross(across).wait_recv()
    for i in range(share):
        summed = part[mine * share + i].astype(jnp.float32) + near[0, i].astype(jnp.float32)
        for across in range(1, pairs):
            summed = summed + arrived[across, i].astype(jnp.float32)
        for t in range(tp):
            base = taken[t, :, i * width : (i + 1) * width].astype(jnp.float32)
            rows = slice(t * own_rows, (t + 1) * own_rows)
            out[rows, i * width : (i + 1) * width] = (base + summed[rows]).astype(jnp.bfloat16)

    swap_state.wait_send()
    swap_total.wait_send()
    for i in range(len(portions)):

        @pl.when(has_above)
        def _():
            carry(i).wait_send()

    def drain(i, c):
        for p in range(cuts):
            for other in range(PAIR if p == crossed else 1):
                chunk = i * PAIR + lax.rem(seat + other, PAIR)
                if p != crossed:
                    relay(chunk, p, side_sems, side).wait_send()

                @pl.when(has_above & (i <= line))
                def _():
                    relay(chunk, p, up_sems, above).wait_send()

                @pl.when(has_below & (i >= line))
                def _():
                    relay(chunk, p, down_sems, below).wait_send()

        return c

    lax.fori_loop(0, lines, drain, 0)
    relay(me, crossed, side_sems, side).wait_send()
    for across in range(pairs):
        to_near(across).wait_send()
        if across:
            to_cross(across).wait_send()
    for step in range(1, tp):
        to_owner(step).wait_send()


def run_mixer(first, second, residual_in, number):
    size, tp = lax.axis_size("sp"), lax.axis_size("tp")
    pairs, share = tp // PAIR, size // tp
    tokens = first[0].shape[0]
    rows, width = first[-1].shape
    cuts = 4
    height = 2 * rows // cuts
    depth = first[2].shape[1] + second[2].shape[1]
    keys = first[0].shape[1] + second[0].shape[1]
    kept = first[2].shape[1] + second[0].shape[1] // LANES * VB
    own_rows, model = residual_in.shape
    half, single, dma = jnp.bfloat16, jnp.float32, pltpu.SemaphoreType.DMA
    return pl.pallas_call(
        functools.partial(mixer_kernel, size, tp),
        out_shape=jax.ShapeDtypeStruct((tokens, model // tp), half),
        in_specs=[VMEM] * 15,
        out_specs=VMEM,
        scratch_shapes=[
            pltpu.VMEM((size, cuts, height, width), half),
            pltpu.VMEM((tokens, depth), single),
            pltpu.VMEM((tokens, keys), single),
            pltpu.VMEM((kept, LANES), single),
            pltpu.VMEM((kept, LANES), half),
            pltpu.VMEM((kept, LANES), half),
            pltpu.VMEM((8, keys), single),
            pltpu.VMEM((8, keys), single),
            pltpu.VMEM((kept, LANES), half),
            pltpu.VMEM((kept, LANES), half),
            pltpu.VMEM((kept, LANES), single),
            pltpu.VMEM((tokens, depth), half),
            pltpu.VMEM((size, tokens, width), half),
            pltpu.VMEM((pairs, share, tokens, width), half),
            pltpu.VMEM((pairs, share, tokens, width), half),
            pltpu.VMEM((pairs, share, tokens, width), half),
            pltpu.VMEM((tp, own_rows, model // tp), half),
            pltpu.VMEM((tp, own_rows, model // tp), half),
        ]
        + [dma((size, cuts))] * 4
        + [dma((1,))] * 4
        + [dma((kept // VB,))] * 2
        + [dma((pairs,))] * 4
        + [dma((tp,))] * 2,
        compiler_params=pltpu.CompilerParams(collective_id=number, has_side_effects=True),
    )(*first, *second, residual_in)


def local_pass(queries, key_rows, values, decay_factors, key_width, value_width):
    count_of_tokens = queries.shape[0]
    head_count = queries.shape[1] // key_width
    blocks = count_of_tokens // BLK
    lower = jnp.tril(jnp.ones((BLK, BLK), jnp.float32))

    def arrange(source, feature_channels):
        return (
            source.astype(jnp.float32)
            .reshape(blocks, BLK, head_count, feature_channels)
            .transpose(0, 2, 1, 3)
        )

    query_blocks = arrange(queries, key_width) * key_width ** (-0.5)
    key_blocks = arrange(key_rows, key_width)
    value_blocks = arrange(values, value_width)
    cumulative = jnp.einsum("ts,nhsd->nhtd", lower, arrange(decay_factors, key_width), precision=highest)
    block_end = cumulative[:, :, -1:, :]
    query_decayed = query_blocks * jnp.exp(cumulative)
    key_inverse = key_blocks * jnp.exp(-cumulative)
    key_to_end = key_blocks * jnp.exp(block_end - cumulative)
    scores = jnp.einsum("nhtd,nhsd->nhts", query_decayed, key_inverse, precision=highest) * lower
    inner = jnp.einsum("nhts,nhsv->nhtv", scores, value_blocks, precision=highest)
    added = jnp.einsum("nhsd,nhsv->nhdv", key_to_end, value_blocks, precision=highest)
    state = jnp.zeros((head_count, key_width, value_width), jnp.float32)
    states = []
    for n in range(blocks):
        states.append(state)
        state = jnp.exp(block_end[n, :, 0])[:, :, None] * state + added[n]
    ends = block_end[:, :, 0]
    return (query_decayed, inner, jnp.stack(states), ends, state)


def finish_pass(query_decayed, inner, states, ends, entering):
    before = jnp.cumsum(ends, axis=0) - ends
    states = states + jnp.exp(before)[:, :, :, None] * entering[None]
    out = inner + jnp.einsum("nhtd,nhdv->nhtv", query_decayed, states, precision=highest)
    blocks, heads, rows, width = out.shape
    return out.transpose(0, 2, 1, 3).reshape(blocks * rows, heads, width)


def entering_state(totals, states, index):
    size = totals.shape[0]
    k = jnp.arange(size)
    reached = (k < index)[:, None]
    masked = jnp.where(reached, totals, 0.0)
    after = (k[None, :] > k[:, None]).astype(jnp.float32)
    behind = jnp.sum(after[:, :, None] * masked[None], axis=1)
    factor = jnp.where(reached, jnp.exp(behind), 0.0)
    return jnp.sum(factor[:, :, None] * states.astype(jnp.float32), axis=0)


def head_norm(attention, head_gain, gate):
    inverse_rms = lax.rsqrt(jnp.mean(attention * attention, axis=-1, keepdims=True) + epsilon)
    gate_silu = jax.nn.silu(gate.astype(jnp.float32).reshape(attention.shape))
    mixed_rows = attention * inverse_rms * head_gain * gate_silu
    return mixed_rows.astype(jnp.bfloat16).reshape(attention.shape[0], -1)


def plain_mixer(first, second, residual_in):
    query_first, key_first, value_first, decay_first, gate_first, norm_first, proj_first = first
    query_second, key_second, value_second, decay_second = second[:4]
    gate_second, norm_second, proj_second = second[4:]
    sp_size, tp_size = lax.axis_size("sp"), lax.axis_size("tp")
    sp_index = lax.axis_index("sp")
    here = local_pass(query_first, key_first, value_first, decay_first, KA, VA)
    there = local_pass(query_second, key_second, value_second, decay_second, KB, VB)
    total_first = jnp.sum(here[3], axis=0).reshape(1, -1)
    total_second = jnp.sum(there[3], axis=0).reshape(1, -1)
    totals = jnp.concatenate((total_first, total_second), axis=1)
    totals = jnp.broadcast_to(totals, (8, totals.shape[1]))
    all_totals, all_first, all_second, *columns = exchange(
        (
            totals,
            here[4].reshape(-1, VA).astype(jnp.bfloat16),
            there[4].reshape(-1, VB).astype(jnp.bfloat16),
            proj_first,
            proj_second,
        ),
        "sp",
        sp_size,
        False,
        0,
    )
    columns = [part.transpose(1, 0, 2).reshape(part.shape[1], -1) for part in columns]
    projection = jnp.concatenate(columns, axis=0)
    cut = total_first.shape[1]
    enter_first = entering_state(all_totals[:, 0, :cut], all_first, sp_index)
    enter_second = entering_state(all_totals[:, 0, cut:], all_second, sp_index)
    attention_first = finish_pass(*here[:4], enter_first.reshape(here[4].shape))
    attention_second = finish_pass(*there[:4], enter_second.reshape(there[4].shape))
    mixed_first = head_norm(attention_first, norm_first, gate_first)
    mixed_second = head_norm(attention_second, norm_second, gate_second)
    mixed_rows = jnp.concatenate((mixed_first, mixed_second), axis=1)
    partial_terms = jnp.dot(mixed_rows, projection, preferred_element_type=jnp.float32)
    block_tokens = query_first.shape[0]
    model_width = partial_terms.shape[1]
    own_tokens = block_tokens // tp_size
    own_columns = model_width // tp_size
    by_owner = (block_tokens, tp_size, own_columns)
    partial_terms = partial_terms.astype(jnp.bfloat16).reshape(by_owner).transpose(1, 0, 2)
    partial_terms = partial_terms.reshape(tp_size, PAIR, block_tokens // PAIR, own_columns)
    mixture = reduce_tp(partial_terms, False, 1).reshape(block_tokens, own_columns)
    own_tokens = residual_in.shape[0]
    residual = residual_in.reshape(own_tokens, tp_size, own_columns).transpose(1, 0, 2)
    (residual,) = exchange((residual,), "tp", tp_size, True, 2)
    residual = residual.reshape(block_tokens, own_columns)
    return (residual.astype(jnp.float32) + mixture).astype(jnp.bfloat16)


def shards(
    query_first,
    key_first,
    value_first,
    decay_first,
    gate_first,
    norm_first,
    proj_first,
    query_second,
    key_second,
    value_second,
    decay_second,
    gate_second,
    norm_second,
    proj_second,
    residual_in,
    expert_norm,
    route_ids,
    route_weight,
    expert_gate,
    expert_up,
    expert_down,
):
    sp_size, tp_size = lax.axis_size("sp"), lax.axis_size("tp")
    first = (query_first, key_first, value_first, decay_first, gate_first)
    first += (norm_first.reshape(1, -1), proj_first)
    second = (query_second, key_second, value_second, decay_second, gate_second)
    second += (norm_second.reshape(1, -1), proj_second)
    whole_lanes = proj_first.shape[1] % LANES == 0 and query_second.shape[1] % LANES == 0
    if whole_lanes and proj_first.shape == proj_second.shape and sp_size == PAIR * tp_size:
        residual = run_mixer(first, second, residual_in, 0)
    else:
        residual = plain_mixer(first, second, residual_in)
    block_tokens, top_count = route_ids.shape
    experts = sp_size
    capacity = 2 * top_count * block_tokens // experts
    return run_experts(
        route_ids,
        route_weight,
        residual,
        expert_norm.reshape(1, -1),
        expert_gate[0],
        expert_up[0],
        expert_down[0],
        capacity,
        3,
    )


def solution(mesh):
    in_specs = (
        P("sp", "tp"),
        P("sp", "tp"),
        P("sp", "tp"),
        P("sp", "tp"),
        P("sp", "tp"),
        P(),
        P("tp", "sp"),
        P("sp", "tp"),
        P("sp", "tp"),
        P("sp", "tp"),
        P("sp", "tp"),
        P("sp", "tp"),
        P(),
        P("tp", "sp"),
        P(("sp", "tp"), None),
        P(),
        P("sp", None),
        P("sp", None),
        P("sp", None, "tp"),
        P("sp", None, "tp"),
        P("sp", "tp", None),
    )
    out_specs = P(("sp", "tp"), None)
    return jax.shard_map(shards, mesh=mesh, in_specs=in_specs, out_specs=out_specs, check_vma=False)
```
